32 devices in a mesh: gr: 2 (over core), fs: 8 (over z, y), tp: 2 (over x).
Axes of the slice: x: 2, y: 2, z: 4, core: 2. Of those that a mesh axis runs over, the one named last changes fastest.
Arguments:
- tokens: bfloat16 [6144, 2048], P(('gr', 'fs')), may hold values from -6 to 6
- route_ids: int32 [6144, 2], P(('gr', 'fs')), may hold values from 0 to 7, as said below
- route_weights: float32 [6144, 2], P(('gr', 'fs')), may hold values from 0.1 to 1
- norm_gain: float32 [2048], P(('gr', 'fs')), may hold values from 0.1 to 1.9
- gate_weight: float32 [8, 2048, 1024], P(None, ('gr', 'fs'), 'tp'), may hold values from -0.125 to 0.125
- up_weight: float32 [8, 2048, 1024], P(None, ('gr', 'fs'), 'tp'), may hold values from -0.125 to 0.125
- down_weight: float32 [8, 1024, 2048], P(None, ('gr', 'fs'), 'tp'), may hold values from -0.1875 to 0.1875
Outputs:
- gate_new: bfloat16 [8, 2048, 1024], P('fs', None, 'tp')
- up_new: bfloat16 [8, 2048, 1024], P('fs', None, 'tp')
- down_new: bfloat16 [8, 1024, 2048], P('fs', 'tp')
- mixed: bfloat16 [6144, 2048], P(('gr', 'fs'), 'tp')
The draws below stay inside these ranges and needn't reach their ends.
Inputs may be any that keep to these rules, and one draw needn't show every extreme that they name: `route_ids`: each row names two different experts of one group (expert e belongs to group e // 2); in each device's block of 384 rows every expert is named by exactly 96 rows.
All inputs are finite; a program needn't handle non-finite values.
Results may differ from the reference program's by a relative error of at most 0.015.
Values may be sent and summed in bfloat16 or wider, within the bound.
A program may use at most 64 MiB of HBM per device.

```python
import jax
import jax.numpy as jnp
from jax import lax

D = 2048
FF = 1024
GROUPS = 4
TOK_DEV = 384
EXPERTS = 8
EPG = 2
HID_DEV = 512
TOKENS = 6144
N_GR = 2
N_FS = 8


def draw_route_ids(key, part):
    blocks = N_GR * N_FS

    def one_block(block_key):
        key_order, key_first, key_step = jax.random.split(block_key, 3)
        place = jax.random.permutation(key_order, TOK_DEV).astype(jnp.int32)
        group = place % GROUPS
        inner = place // GROUPS
        first_shift = jax.random.randint(key_first, (GROUPS,), 0, EPG).astype(jnp.int32)
        step_shift = jax.random.randint(key_step, (GROUPS,), 0, EPG - 1).astype(jnp.int32)
        first = (inner + first_shift[group]) % EPG
        stride = 1 + (inner // EPG + step_shift[group]) % (EPG - 1)
        second = (first + stride) % EPG
        return jnp.stack([group * EPG + first, group * EPG + second], axis=1).astype(jnp.int32)
    keys = jax.random.split(key, blocks)
    return jax.vmap(one_block)(keys).reshape(TOKENS, 2)


def shard_levels(stream_key, shape, cuts, low, top_value):
    gain, own = 1.0, jax.random.fold_in(stream_key, 6)
    for position, shards_of in cuts:
        draws = jnp.exp(jax.random.uniform(jax.random.fold_in(own, position), (shards_of,), jnp.float32, low / len(cuts), top_value / len(cuts)))
        gain = gain * jnp.repeat(draws, shape[position] // shards_of).reshape([-1 if axis == position else 1 for axis in range(len(shape))])
    return gain


def gaussian(own_key, shape, width, limit, cuts=(), held_as=jnp.bfloat16):
    level = shard_levels(own_key, shape, cuts, -0.22, 0.18) if cuts else 1.0
    array = jax.random.normal(own_key, shape, jnp.float32) * width * level
    return jnp.minimum(jnp.maximum(array, -limit), limit).astype(held_as)


def setup_inputs(seed: int = 0) -> dict:
    arg_keys = jax.random.split(jax.random.key(seed), 8)
    return {
        "tokens": gaussian(arg_keys[0], (TOKENS, D), 1.0, 6.0, ((0, 16),)),
        "route_ids": draw_route_ids(jax.random.fold_in(arg_keys[7], 71), 0),
        "route_weights": jnp.clip(0.1 + 0.9 * jax.random.uniform(arg_keys[2], (TOKENS, 2), jnp.float32) ** shard_levels(arg_keys[2], (TOKENS, 2), ((0, 16),), -0.2, 0.2), 0.1, 1.0),
        "norm_gain": jnp.clip(1.0 + 0.18 * jax.random.normal(arg_keys[3], (D,), jnp.float32), 0.1, 1.9),
        "gate_weight": gaussian(arg_keys[4], (EXPERTS, D, FF), D ** -0.5, 0.125, ((1, 16), (2, 2)), jnp.float32),
        "up_weight": gaussian(arg_keys[5], (EXPERTS, D, FF), D ** -0.5, 0.125, ((1, 16), (2, 2)), jnp.float32),
        "down_weight": gaussian(arg_keys[6], (EXPERTS, FF, D), FF ** -0.5, 0.1875, ((1, 16), (2, 2)), jnp.float32),
    }


def expert_block(args):
    gate_one, up_one, down_one, rows = args
    first = jnp.dot(rows, gate_one, preferred_element_type=jnp.float32)
    second = jnp.dot(rows, up_one, preferred_element_type=jnp.float32)
    hidden = (jax.nn.silu(first) * second).astype(jnp.bfloat16)
    count = rows.shape[0]
    pieces = hidden.reshape(count, FF // HID_DEV, HID_DEV).astype(jnp.float32)
    down_pieces = down_one.reshape(FF // HID_DEV, HID_DEV, D).astype(jnp.float32)
    partials = jnp.einsum('mbf,bfd->bmd', pieces, down_pieces).astype(jnp.bfloat16)
    return lax.optimization_barrier(jnp.sum(partials.astype(jnp.float32), axis=0)).astype(jnp.bfloat16)

def reference(tokens, route_ids, route_weights, norm_gain, gate_weight, up_weight, down_weight):
    gate_new = (gate_weight * norm_gain[None, :, None]).astype(jnp.bfloat16)
    up_new = (up_weight * norm_gain[None, :, None]).astype(jnp.bfloat16)
    down_new = down_weight.astype(jnp.bfloat16)
    widened = tokens.astype(jnp.float32)
    normed = (widened * lax.rsqrt(lax.optimization_barrier(jnp.mean(widened * widened, axis=-1, keepdims=True)) + 1e-06)).astype(jnp.bfloat16)
    flat_ids = route_ids.reshape(-1)
    per_expert = flat_ids.shape[0] // EXPERTS
    order = jnp.argsort(flat_ids, stable=True).astype(jnp.int32).reshape(EXPERTS, per_expert)

    def one_expert(args):
        gate_one, up_one, down_one, picks = args
        rows = normed[picks // 2]
        return expert_block((gate_one, up_one, down_one, rows))
    results = lax.map(one_expert, (gate_new, up_new, down_new, order))
    route_out = jnp.zeros((flat_ids.shape[0], D), jnp.bfloat16).at[order.reshape(-1)].set(results.reshape(-1, D))
    route_out = route_out.reshape(-1, 2, D).astype(jnp.float32)
    mixed = lax.optimization_barrier(jnp.sum(route_weights[:, :, None] * route_out, axis=1)).astype(jnp.bfloat16)
    return (gate_new, up_new, down_new, mixed)
```

```python
import functools

import jax
import jax.numpy as jnp
from jax import lax
from jax.experimental import pallas as pl
from jax.experimental.pallas import tpu as pltpu
from jax.sharding import PartitionSpec as P

GROUPS = 4
HEAD = 2
HALVES = 2
RETURN = (3, 2, 1, 0)
BF16 = jnp.bfloat16
MESH = pl.DeviceIdType.MESH


def local(tokens, route_ids, route_weights, norm_gain, gate_weight, up_weight, down_weight):
    gate_folded = (gate_weight * norm_gain[None, :, None]).astype(jnp.bfloat16)
    up_folded = (up_weight * norm_gain[None, :, None]).astype(jnp.bfloat16)
    down_rounded = down_weight.astype(jnp.bfloat16)
    moved = (
        lax.all_to_all(gate_folded, "fs", split_axis=0, concat_axis=1, tiled=True),
        lax.all_to_all(up_folded, "fs", split_axis=0, concat_axis=1, tiled=True),
        lax.all_to_all(down_rounded, "fs", split_axis=0, concat_axis=1, tiled=True),
    )
    gate_new, up_new, down_whole = (
        lax.all_gather(moved[0], "gr", axis=1, tiled=True),
        lax.all_gather(moved[1], "gr", axis=1, tiled=True),
        lax.all_gather(moved[2], "gr", axis=1, tiled=True),
    )
    down_new = lax.all_to_all(down_whole, "tp", split_axis=1, concat_axis=2, tiled=True)
    tok = tokens.shape[0]
    width = tokens.shape[1]
    experts = gate_weight.shape[0]
    cap = 2 * tok // experts
    flat_ids = route_ids.reshape(-1)
    onehot = (flat_ids[:, None] == jnp.arange(experts, dtype=jnp.int32)[None, :]).astype(jnp.int32)
    slot = jnp.sum(jnp.cumsum(onehot, axis=0) * onehot, axis=1) - 1
    position = flat_ids * cap + slot
    source = (
        jnp.zeros((experts * cap,), jnp.int32)
        .at[position]
        .set(jnp.arange(2 * tok, dtype=jnp.int32) // 2)
    )
    widened = tokens.astype(jnp.float32)
    normed = (
        widened * lax.rsqrt(jnp.mean(widened * widened, axis=-1, keepdims=True) + 1e-06)
    ).astype(jnp.bfloat16)
    outgoing = normed[source].reshape(experts, cap, width)
    received = lax.all_to_all(outgoing, "fs", split_axis=0, concat_axis=0, tiled=True)
    senders, count, _ = received.shape
    rows = received.reshape(senders * count, width)
    first = jnp.dot(rows, gate_new[0], preferred_element_type=jnp.float32)
    second = jnp.dot(rows, up_new[0], preferred_element_type=jnp.float32)
    hidden = (jax.nn.silu(first) * second).astype(jnp.bfloat16)
    partial_out = jnp.dot(hidden, down_new[0], preferred_element_type=jnp.float32)
    summed = lax.psum_scatter(
        partial_out.reshape(senders, count, width).astype(jnp.bfloat16),
        "tp",
        scatter_dimension=2,
        tiled=True,
    )
    returned = lax.all_to_all(summed, "fs", split_axis=0, concat_axis=0, tiled=True)
    columns = returned.shape[2]
    route_out = returned.reshape(experts * cap, columns)[position].reshape(tok, 2, columns)
    mixed = jnp.sum(route_weights[:, :, None] * route_out.astype(jnp.float32), axis=1).astype(
        jnp.bfloat16
    )
    return (gate_new, up_new, down_new, mixed)


def place(n_z, n_y):
    f = lax.axis_index("fs")
    return lax.axis_index("gr"), f // n_y, lax.rem(f, n_y), lax.axis_index("tp")


def flip(z, k):
    return (z, z + 1 - 2 * lax.rem(z, 2), lax.rem(z + 2, 4), 3 - z)[k]


def device(c, z, y, x, n_y):
    return {"gr": c, "fs": z * n_y + y, "tp": x}


def greet(peers):
    barrier = pltpu.get_barrier_semaphore()
    for peer in peers:
        pl.semaphore_signal(barrier, inc=1, device_id=peer, device_id_type=MESH)
    return lambda: pl.semaphore_wait(barrier, len(peers))


def remote(src, dst, send, recv, peer):
    return pltpu.make_async_remote_copy(
        src_ref=src, dst_ref=dst, send_sem=send, recv_sem=recv,
        device_id=peer, device_id_type=MESH,
    )


def landed(ref, sem):
    pltpu.make_async_copy(ref, ref, sem).wait()


def sampler(
    n_z, n_y,
    tok_hbm, ids_hbm, rw_hbm, gain_hbm, gate_in, up_in, down_in,
    land, dland, dcross, ret, spot,
    tok_in, ids_in, rw_in, gain_in, wide, narrow, dwide, dnarrow,
    normed, tok_s, rows, rw_s, rw_l, hid, out_s, ry_l, fin,
    in_sem, ld_sem, dl_sem, w_send, w_recv, f_send, f_recv,
    tz_send, tz_recv, ty_send, ty_recv, tx_send, tx_recv,
    rz_send, rz_recv, ry_send, ry_recv,
    h_send, h_recv, c_send, c_recv, y_send, y_recv, z_send, z_recv,
):
    c, z, y, x = place(n_z, n_y)
    me = z * n_y + y
    n_fs = n_z * n_y
    g_rows, d_rows = gate_in.shape[1], down_in.shape[1]
    tok, width = tok_in.shape
    half = width // 2
    cap = tok // GROUPS
    hb = n_fs * d_rows
    q = hb // HALVES
    piece = half // HALVES
    f32 = jnp.float32
    dev = functools.partial(device, n_y=n_y)
    ks = [(kz, 0) for kz in (3, 2, 1)] + [(kz, 1) for kz in (3, 2, 1, 0)] + [(0, 0)]
    last = len(ks) - 1
    at = []
    for kz, ky in ks:
        pz, py = flip(z, kz), (1 - y if ky else y)
        at.append((pz * n_y + py, dev(c, pz, py, x)))
    other = dev(1 - c, z, y, x)
    x_nbr = dev(c, z, y, 1 - x)
    y_nbr = dev(c, z, 1 - y, x)

    def xcols(i):
        return pl.ds(pl.multiple_of(i * half, half), half)

    def grow(core, f):
        return pl.ds(pl.multiple_of((core * n_fs + f) * g_rows, g_rows), g_rows)

    def drow(core, f):
        return pl.ds(pl.multiple_of((core * n_fs + f) * d_rows, d_rows), d_rows)

    def core_rows(core, count):
        return pl.ds(pl.multiple_of(core * n_fs * count, n_fs * count), n_fs * count)

    def trow(f):
        return pl.ds(pl.multiple_of(f * cap, cap), cap)

    met = greet([d for _, d in at[:last]] + [other, x_nbr])
    small = []

    def fetch(src, dst):
        cp = pltpu.make_async_copy(src, dst, in_sem.at[len(small)])
        cp.start()
        small.append(cp)

    fetch(gain_hbm, gain_in)
    loads = {}

    def load(n):
        for i, ref in enumerate((gate_in, up_in)):
            pltpu.make_async_copy(ref.at[at[n][0]], wide.at[n, i], ld_sem.at[n]).start()

    for n in range(HEAD):
        load(n)
    fetch(tok_hbm, tok_in)
    fetch(ids_hbm, ids_in)
    fetch(rw_hbm, rw_in)
    for n in range(HEAD, last + 1):
        load(n)
    for n, (p, _) in enumerate(at):
        pltpu.make_async_copy(down_in.at[p], dwide.at[n], dl_sem.at[0]).start()

    def column(row, count):
        lanes = row.shape[1]
        eye = (lax.broadcasted_iota(jnp.int32, (count, lanes), 0)
               == lax.broadcasted_iota(jnp.int32, (count, lanes), 1))
        return jnp.sum(jnp.where(eye, row, 0.0), axis=1, keepdims=True)

    small[0].wait()
    gain = column(gain_in[...], g_rows)

    def fold(n):
        landed(wide.at[n], ld_sem.at[n])
        for i in range(2):
            value = (wide[n, i] * gain).astype(BF16)
            for a in range(HALVES):
                part = value[:, a * q:(a + 1) * q]
                if n == last:
                    land[a, i, grow(c, me), :] = part
                else:
                    narrow[n, a, i] = part

    arrive = {}
    onward = {}

    def forward(n, a):
        block = land.at[a, :, grow(c, at[n][0]), :]
        onward[n, a] = remote(block, block, f_send.at[0], f_recv.at[a], other)
        onward[n, a].start()

    def spread(n, a):
        if n == last:
            forward(n, a)
        else:
            arrive[n, a] = remote(narrow.at[n, a], land.at[a, :, grow(c, me), :],
                                  w_send.at[0], w_recv.at[a, n], at[n][1])
            arrive[n, a].start()

    for n in range(HEAD):
        fold(n)
    met()
    for n in range(HEAD):
        spread(n, 0)

    for cp in small[1:]:
        cp.wait()

    def norm_rows(i, carry):
        r = pl.ds(pl.multiple_of(i * cap, cap), cap)
        v = tok_in[r, :].astype(f32)
        scale = lax.rsqrt(jnp.mean(v * v, axis=-1, keepdims=True) + 1e-06)
        normed[r, :] = (tok_in[r, xcols(x)].astype(f32) * scale).astype(BF16)
        return carry

    lax.fori_loop(0, GROUPS, norm_rows, 0)
    epg = gate_in.shape[0] // GROUPS
    low = ids_in[0:1, :]
    group = jnp.zeros_like(low)
    for g in range(1, GROUPS):
        group += (low >= g * epg).astype(jnp.int32)
    ahead = low == group * epg
    w_a, w_b = rw_in[0:1, :], rw_in[1:2, :]
    sub = lax.broadcasted_iota(jnp.int32, (8, tok), 0)
    w_of = jnp.where(sub == 0, jnp.where(ahead, w_a, w_b),
                     jnp.where(sub == 1, jnp.where(ahead, w_b, w_a), 0.0))
    onehot = (lax.broadcasted_iota(jnp.int32, (8, tok), 0) == group).astype(f32)
    upto = (lax.broadcasted_iota(jnp.int32, (tok, tok), 0)
            <= lax.broadcasted_iota(jnp.int32, (tok, tok), 1)).astype(BF16)
    count = jnp.dot(onehot.astype(BF16), upto, preferred_element_type=f32)
    slot = jnp.sum(onehot * count, axis=0, keepdims=True).astype(jnp.int32) - 1
    position = group * cap + slot
    spot[...] = jnp.broadcast_to(position, spot.shape)

    def picked(g):
        return lax.broadcasted_iota(jnp.int32, (cap, tok), 0) + g * cap == position

    tz, rz, ty, tx, ry = {}, {}, {}, {}, {}
    for kz in (3, 2, 1, 0):
        g = flip(z, kz)
        pick = picked(g)
        block = jnp.dot(pick.astype(BF16), normed[...], preferred_element_type=f32).astype(BF16)
        w_row = lax.dot_general(w_of, pick.astype(f32), (((1,), (1,)), ((), ())),
                                precision=lax.Precision.HIGHEST, preferred_element_type=f32)
        if kz:
            tok_s[kz - 1] = block
            rw_s[kz - 1, :, :cap] = w_row
            peer = dev(c, g, y, x)
            tz[kz] = remote(tok_s.at[kz - 1], rows.at[trow(me), xcols(x)],
                            tz_send.at[0], tz_recv.at[kz - 1], peer)
            tz[kz].start()
            rz[kz] = remote(rw_s.at[kz - 1], rw_l.at[y, z], rz_send.at[0], rz_recv.at[kz - 1], peer)
            rz[kz].start()
        else:
            rows[trow(me), xcols(x)] = block
            rw_l[y, z, :, :cap] = w_row

    def pass_x(f):
        block = rows.at[trow(f), xcols(x)]
        tx[len(tx)] = remote(block, block, tx_send.at[0], tx_recv.at[0], x_nbr)
        tx[len(tx) - 1].start()

    def pass_on(kz):
        zs = flip(z, kz)
        src = zs * n_y + y
        block = rows.at[trow(src), xcols(x)]
        ty[kz] = remote(block, block, ty_send.at[0], ty_recv.at[kz], y_nbr)
        ty[kz].start()
        pass_x(src)
        ry[kz] = remote(rw_l.at[y, zs], rw_l.at[y, zs], ry_send.at[0], ry_recv.at[0], y_nbr)
        ry[kz].start()

    pass_on(0)
    for n in range(HEAD, last + 1):
        fold(n)
        spread(n, 0)
    for n in range(last + 1):
        spread(n, 1)

    landed(dwide, dl_sem.at[0])

    def dforward(n, h):
        block = dland.at[h, drow(c, at[n][0])]
        onward[n, 2 + h] = remote(block, block, f_send.at[1], f_recv.at[2 + h], other)
        onward[n, 2 + h].start()

    for h in range(HALVES):
        for n in range(last + 1):
            value = dwide[n, :, h * piece:(h + 1) * piece].astype(BF16)
            if n == last:
                dland[h, drow(c, me)] = value
                dforward(n, h)
            else:
                dnarrow[h, n] = value
                arrive[n, 2 + h] = remote(dnarrow.at[h, n], dland.at[h, drow(c, me)],
                                          w_send.at[1], w_recv.at[2 + h, n], at[n][1])
                arrive[n, 2 + h].start()

    for kz in (1, 3, 2):
        tz[kz].wait_recv()
        rz[kz].wait_recv()
        pass_on(kz)
    for kz in (0, 1, 3, 2):
        ty[kz].wait_recv()
        pass_x(flip(z, kz) * n_y + 1 - y)

    order = sorted(range(last), key=lambda n: ks[n])

    def gather(a):
        for n in order:
            arrive[n, a].wait_recv()
            forward(n, a)
        if a == 0:
            landed(rows.at[:, xcols(1 - x)], tx_recv.at[0])
            landed(rw_l.at[1 - y], ry_recv.at[0])
        landed(land.at[a, :, core_rows(1 - c, g_rows), :], f_recv.at[a])

    m = n_y * cap
    hsend = {}
    for a in range(HALVES):
        gather(a)
        for n, kz in enumerate(RETURN):
            r = pl.ds(pl.multiple_of(flip(z, kz) * m, m), m)
            v = jnp.dot(rows[r, :], land[a, 0], preferred_element_type=f32)
            w = jnp.dot(rows[r, :], land[a, 1], preferred_element_type=f32)
            hid[x, a, r, :] = (v / (1.0 + jnp.exp(-v)) * w).astype(BF16)
            cp = remote(hid.at[x, a, r], hid.at[x, a, r], h_send.at[0], h_recv.at[a, n], x_nbr)
            cp.start()
            hsend[a, n] = cp

    part = hb // 2
    mine = pl.ds(pl.multiple_of(c * part, part), part)
    cross = []
    ysend = {}
    zsend = {}

    def give_back(n, h):
        kz = RETURN[n]
        ysend[n, h].wait_recv()
        total = (out_s[h, n, 1].astype(f32) + ry_l[h, n].astype(f32)).astype(BF16)
        d = pl.ds(h * piece, piece)
        if kz:
            fin[h, n] = total
            zsend[n, h] = remote(fin.at[h, n], ret.at[trow(z), d], z_send.at[0], z_recv.at[h],
                                 dev(c, flip(z, kz), y, x))
            zsend[n, h].start()
        else:
            ret[trow(z), d] = total

    for h in range(HALVES):
        for n in order:
            arrive[n, 2 + h].wait_recv()
            dforward(n, h)
        landed(dland.at[h, core_rows(1 - c, d_rows)], f_recv.at[2 + h])
        cp = remote(dland.at[h, pl.ds(pl.multiple_of((1 - x) * hb + c * part, part), part)],
                    dcross.at[h, mine], c_send.at[0], c_recv.at[h], x_nbr)
        for n, kz in enumerate(RETURN):
            zs = flip(z, kz)
            if h == 0:
                for a in range(HALVES):
                    hsend[a, n].wait_recv()
            for step in range(2):
                s = 1 - y if step == 0 else y
                f = zs * n_y + s
                w = jnp.where(y == 0, rw_l[s, zs, 0:1, :], rw_l[s, zs, 1:2, :])
                lane = lax.broadcasted_iota(jnp.int32, w.shape, 1)
                w = column(jnp.where(lane < cap, w, 0.0), cap)
                acc = jnp.zeros((cap, piece), f32)
                for i in range(2):
                    for a in range(HALVES):
                        acc += jnp.dot(hid[i, a, trow(f)], dland[h, pl.ds(i * hb + a * q, q)],
                                       preferred_element_type=f32)
                out_s[h, n, step] = (acc * w).astype(BF16)
                if step == 0:
                    ysend[n, h] = remote(out_s.at[h, n, 0], ry_l.at[h, n],
                                         y_send.at[0], y_recv.at[h, n], y_nbr)
                    ysend[n, h].start()
            if n:
                give_back(n - 1, h)
        cp.start()
        cross.append(cp)
        give_back(len(RETURN) - 1, h)

    over = []
    for h in range(HALVES):
        cross[h].wait_recv()
        block = dcross.at[h, mine]
        cp = remote(block, block, c_send.at[1], c_recv.at[2 + h], other)
        cp.start()
        over.append(cp)
    for h in range(HALVES):
        landed(fin.at[h, pl.ds(0, GROUPS - 1)], z_recv.at[h])
    for cp in over:
        cp.wait_recv()
    landed(narrow, w_send.at[0])
    landed(dnarrow, w_send.at[1])
    landed(land.at[:, :, core_rows(c, g_rows), :], f_send.at[0])
    landed(dland.at[:, core_rows(c, d_rows)], f_send.at[1])
    landed(tok_s, tz_send.at[0])
    landed(rw_s, rz_send.at[0])
    landed(rw_l.at[y], ry_send.at[0])
    landed(fin, ty_send.at[0])
    landed(rows.at[:, xcols(x)], tx_send.at[0])
    landed(hid.at[x], h_send.at[0])
    landed(dcross.at[:, mine], c_send.at[0])
    landed(dcross.at[:, mine], c_send.at[1])
    landed(ry_l, y_send.at[0])
    landed(fin.at[:, pl.ds(0, GROUPS - 1)], z_send.at[0])


def finish(n_z, n_y, land, dland, dcross, ret, spot, gate_out, up_out, down_out, mixed_out, mixed, sem):
    x = place(n_z, n_y)[3]
    tok, half = ret.shape
    hb, piece = dcross.shape[1:]
    q = land.shape[3]
    copies = []

    def put(src, dst):
        cp = pltpu.make_async_copy(src, dst, sem.at[len(copies)])
        cp.start()
        copies.append(cp)

    for i, out in enumerate((gate_out, up_out)):
        for a in range(HALVES):
            put(land.at[a, i], out.at[0, :, pl.ds(a * q, q)])
    for h in range(HALVES):
        put(dland.at[h, pl.ds(pl.multiple_of(x * hb, hb), hb)],
            down_out.at[0, :, pl.ds(pl.multiple_of(x * half + h * piece, piece), piece)])
        put(dcross.at[h],
            down_out.at[0, :, pl.ds(pl.multiple_of((1 - x) * half + h * piece, piece), piece)])
    everyone = (lax.broadcasted_iota(jnp.int32, (tok, tok), 0) == spot[0:1, :]).astype(BF16)
    mixed[...] = lax.dot_general(
        everyone, ret[...], (((0,), (0,)), ((), ())), preferred_element_type=jnp.float32).astype(BF16)
    put(mixed, mixed_out)
    for cp in copies:
        cp.wait()


def paired(n_z, n_y, tokens, route_ids, route_weights, norm_gain, gate_weight, up_weight, down_weight):
    tok, width = tokens.shape
    cap = tok // GROUPS
    half = width // lax.axis_size("tp")
    n_fs = n_z * n_y
    d_rows, d_cols = down_weight.shape[1:]
    g_rows, g_cols = gate_weight.shape[1:]
    f32, i32 = jnp.float32, jnp.int32
    q, piece = g_cols // HALVES, half // HALVES
    hb = n_fs * d_rows

    hbm = pl.BlockSpec(memory_space=pltpu.HBM)
    vmem = pl.BlockSpec(memory_space=pltpu.VMEM)
    dma = pltpu.SemaphoreType.DMA
    lanes = -(-cap // 128) * 128
    held = pl.pallas_call(
        functools.partial(sampler, n_z, n_y),
        out_shape=(
            pltpu.VMEM((HALVES, 2, 2 * n_fs * g_rows, q), BF16),
            pltpu.VMEM((HALVES, 2 * hb, piece), BF16),
            pltpu.VMEM((HALVES, hb, piece), BF16),
            pltpu.VMEM((tok, half), BF16),
            pltpu.VMEM((8, tok), i32),
        ),
        in_specs=[hbm] * 7,
        out_specs=(vmem,) * 5,
        scratch_shapes=[
            pltpu.VMEM((tok, width), BF16),
            pltpu.VMEM((2, tok), i32),
            pltpu.VMEM((2, tok), f32),
            pltpu.VMEM((1, g_rows), f32),
            pltpu.VMEM((n_fs, 2, g_rows, g_cols), f32),
            pltpu.VMEM((n_fs - 1, HALVES, 2, g_rows, q), BF16),
            pltpu.VMEM((n_fs, d_rows, d_cols), f32),
            pltpu.VMEM((HALVES, n_fs - 1, d_rows, piece), BF16),
            pltpu.VMEM((tok, half), BF16),
            pltpu.VMEM((3, cap, half), BF16),
            pltpu.VMEM((n_fs * cap, width), BF16),
            pltpu.VMEM((3, 8, lanes), f32),
            pltpu.VMEM((n_y, n_z, 8, lanes), f32),
            pltpu.VMEM((2, HALVES, n_fs * cap, q), BF16),
            pltpu.VMEM((HALVES, 4, 2, cap, piece), BF16),
            pltpu.VMEM((HALVES, 4, cap, piece), BF16),
            pltpu.VMEM((HALVES, 4, cap, piece), BF16),
            dma((4,)), dma((n_fs,)), dma((1,)),
            dma((2,)), dma((4, n_fs - 1)), dma((2,)), dma((4,)),
            dma((1,)), dma((3,)), dma((1,)), dma((4,)), dma((1,)), dma((1,)),
            dma((1,)), dma((3,)), dma((1,)), dma((1,)),
            dma((1,)), dma((HALVES, 4)), dma((2,)), dma((4,)),
            dma((1,)), dma((HALVES, 4)), dma((1,)), dma((2,)),
        ],
        compiler_params=pltpu.CompilerParams(
            collective_id=0, has_side_effects=True, vmem_limit_bytes=40 * 1024 * 1024),
    )(*(pltpu.with_memory_space_constraint(v, pltpu.HBM) for v in (
        tokens, route_ids.T, route_weights.T, norm_gain.reshape(1, g_rows),
        gate_weight, up_weight, down_weight)))
    return pl.pallas_call(
        functools.partial(finish, n_z, n_y),
        out_shape=(
            jax.ShapeDtypeStruct((1, 2 * n_fs * g_rows, g_cols), BF16),
            jax.ShapeDtypeStruct((1, 2 * n_fs * g_rows, g_cols), BF16),
            jax.ShapeDtypeStruct((1, hb, 2 * d_cols), BF16),
            jax.ShapeDtypeStruct((tok, half), BF16),
        ),
        in_specs=[vmem] * 5,
        out_specs=(hbm,) * 4,
        scratch_shapes=[pltpu.VMEM((tok, half), BF16), dma((9,))],
        compiler_params=pltpu.CompilerParams(vmem_limit_bytes=8 * 1024 * 1024),
    )(*(pltpu.with_memory_space_constraint(v, pltpu.VMEM) for v in held))


def solution(mesh):
    placed = (
        P(("gr", "fs"), None),
        P(("gr", "fs"), None),
        P(("gr", "fs"), None),
        P(("gr", "fs")),
        P(None, ("gr", "fs"), "tp"),
        P(None, ("gr", "fs"), "tp"),
        P(None, ("gr", "fs"), "tp"),
    )
    n_fs = mesh.shape["fs"]

    def body(*args):
        experts = args[4].shape[0]
        if experts == n_fs == 2 * GROUPS and mesh.shape["gr"] == mesh.shape["tp"] == 2:
            return paired(GROUPS, 2, *args)
        return local(*args)

    return jax.shard_map(
        body,
        mesh=mesh,
        in_specs=placed,
        out_specs=(
            P("fs", None, "tp"),
            P("fs", None, "tp"),
            P("fs", "tp", None),
            P(("gr", "fs"), "tp"),
        ),
        check_vma=False,
    )
```

```python
import functools

import jax
import jax.numpy as jnp
from jax import lax
from jax.experimental import pallas as pl
from jax.experimental.pallas import tpu as pltpu
from jax.sharding import PartitionSpec as P

GROUPS = 4
HEAD = 2
HALVES = 2
RETURN = (3, 2, 1, 0)
BF16 = jnp.bfloat16
MESH = pl.DeviceIdType.MESH


def local(tokens, route_ids, route_weights, norm_gain, gate_weight, up_weight, down_weight):
    gate_folded = (gate_weight * norm_gain[None, :, None]).astype(jnp.bfloat16)
    up_folded = (up_weight * norm_gain[None, :, None]).astype(jnp.bfloat16)
    down_rounded = down_weight.astype(jnp.bfloat16)
    moved = (
        lax.all_to_all(gate_folded, "fs", split_axis=0, concat_axis=1, tiled=True),
        lax.all_to_all(up_folded, "fs", split_axis=0, concat_axis=1, tiled=True),
        lax.all_to_all(down_rounded, "fs", split_axis=0, concat_axis=1, tiled=True),
    )
    gate_new, up_new, down_whole = (
        lax.all_gather(moved[0], "gr", axis=1, tiled=True),
        lax.all_gather(moved[1], "gr", axis=1, tiled=True),
        lax.all_gather(moved[2], "gr", axis=1, tiled=True),
    )
    down_new = lax.all_to_all(down_whole, "tp", split_axis=1, concat_axis=2, tiled=True)
    tok = tokens.shape[0]
    width = tokens.shape[1]
    experts = gate_weight.shape[0]
    cap = 2 * tok // experts
    flat_ids = route_ids.reshape(-1)
    onehot = (flat_ids[:, None] == jnp.arange(experts, dtype=jnp.int32)[None, :]).astype(jnp.int32)
    slot = jnp.sum(jnp.cumsum(onehot, axis=0) * onehot, axis=1) - 1
    position = flat_ids * cap + slot
    source = (
        jnp.zeros((experts * cap,), jnp.int32)
        .at[position]
        .set(jnp.arange(2 * tok, dtype=jnp.int32) // 2)
    )
    widened = tokens.astype(jnp.float32)
    normed = (
        widened * lax.rsqrt(jnp.mean(widened * widened, axis=-1, keepdims=True) + 1e-06)
    ).astype(jnp.bfloat16)
    outgoing = normed[source].reshape(experts, cap, width)
    received = lax.all_to_all(outgoing, "fs", split_axis=0, concat_axis=0, tiled=True)
    senders, count, _ = received.shape
    rows = received.reshape(senders * count, width)
    first = jnp.dot(rows, gate_new[0], preferred_element_type=jnp.float32)
    second = jnp.dot(rows, up_new[0], preferred_element_type=jnp.float32)
    hidden = (jax.nn.silu(first) * second).astype(jnp.bfloat16)
    partial_out = jnp.dot(hidden, down_new[0], preferred_element_type=jnp.float32)
    summed = lax.psum_scatter(
        partial_out.reshape(senders, count, width).astype(jnp.bfloat16),
        "tp",
        scatter_dimension=2,
        tiled=True,
    )
    returned = lax.all_to_all(summed, "fs", split_axis=0, concat_axis=0, tiled=True)
    columns = returned.shape[2]
    route_out = returned.reshape(experts * cap, columns)[position].reshape(tok, 2, columns)
    mixed = jnp.sum(route_weights[:, :, None] * route_out.astype(jnp.float32), axis=1).astype(
        jnp.bfloat16
    )
    return (gate_new, up_new, down_new, mixed)


def place(n_z, n_y):
    f = lax.axis_index("fs")
    return lax.axis_index("gr"), f // n_y, lax.rem(f, n_y), lax.axis_index("tp")


def flip(z, k):
    return (z, z + 1 - 2 * lax.rem(z, 2), lax.rem(z + 2, 4), 3 - z)[k]


def device(c, z, y, x, n_y):
    return {"gr": c, "fs": z * n_y + y, "tp": x}


def greet(peers):
    barrier = pltpu.get_barrier_semaphore()
    for peer in peers:
        pl.semaphore_signal(barrier, inc=1, device_id=peer, device_id_type=MESH)
    return lambda: pl.semaphore_wait(barrier, len(peers))


def remote(src, dst, send, recv, peer):
    return pltpu.make_async_remote_copy(
        src_ref=src, dst_ref=dst, send_sem=send, recv_sem=recv,
        device_id=peer, device_id_type=MESH,
    )


def landed(ref, sem):
    pltpu.make_async_copy(ref, ref, sem).wait()


def sampler(
    n_z, n_y,
    tok_hbm, ids_hbm, rw_hbm, gain_hbm, gate_in, up_in, down_in,
    land, dland, dcross, ret, spot,
    tok_in, ids_in, rw_in, gain_in, wide, narrow, dwide, dnarrow,
    normed, tok_s, rows, rw_s, rw_l, hid, out_s, ry_l, fin,
    in_sem, ld_sem, dl_sem, w_send, w_recv, f_send, f_recv,
    tz_send, tz_recv, ty_send, ty_recv, tx_send, tx_recv,
    rz_send, rz_recv, ry_send, ry_recv,
    h_send, h_recv, c_send, c_recv, y_send, y_recv, z_send, z_recv,
):
    c, z, y, x = place(n_z, n_y)
    me = z * n_y + y
    n_fs = n_z * n_y
    g_rows, d_rows = gate_in.shape[1], down_in.shape[1]
    tok, width = tok_in.shape
    half = width // 2
    cap = tok // GROUPS
    hb = n_fs * d_rows
    q = hb // HALVES
    piece = half // HALVES
    f32 = jnp.float32
    dev = functools.partial(device, n_y=n_y)
    ks = [(kz, ky) for kz in (3, 2, 1) for ky in (0, 1)] + [(0, 1), (0, 0)]
    last = len(ks) - 1
    at = []
    for kz, ky in ks:
        pz = flip(z, kz)
        py = lax.rem(y + ky + c, 2) if kz else (1 - y if ky else y)
        at.append((pz * n_y + py, dev(c, pz, py, x)))
    other = dev(1 - c, z, y, x)
    x_nbr = dev(c, z, y, 1 - x)
    y_nbr = dev(c, z, 1 - y, x)

    def xcols(i):
        return pl.ds(pl.multiple_of(i * half, half), half)

    def grow(core, f):
        return pl.ds(pl.multiple_of((core * n_fs + f) * g_rows, g_rows), g_rows)

    def drow(core, f):
        return pl.ds(pl.multiple_of((core * n_fs + f) * d_rows, d_rows), d_rows)

    def core_rows(core, count):
        return pl.ds(pl.multiple_of(core * n_fs * count, n_fs * count), n_fs * count)

    def trow(f):
        return pl.ds(pl.multiple_of(f * cap, cap), cap)

    met = greet([d for _, d in at[:last]] + [other, x_nbr])
    small = []

    def fetch(src, dst):
        cp = pltpu.make_async_copy(src, dst, in_sem.at[len(small)])
        cp.start()
        small.append(cp)

    fetch(gain_hbm, gain_in)
    loads = {}

    def load(n):
        for i, ref in enumerate((gate_in, up_in)):
            pltpu.make_async_copy(ref.at[at[n][0]], wide.at[n, i], ld_sem.at[n]).start()

    for n in range(HEAD):
        load(n)
    fetch(tok_hbm, tok_in)
    fetch(ids_hbm, ids_in)
    fetch(rw_hbm, rw_in)
    for n in range(HEAD, last + 1):
        load(n)
    for n, (p, _) in enumerate(at):
        pltpu.make_async_copy(down_in.at[p], dwide.at[n], dl_sem.at[0]).start()

    def column(row, count):
        lanes = row.shape[1]
        eye = (lax.broadcasted_iota(jnp.int32, (count, lanes), 0)
               == lax.broadcasted_iota(jnp.int32, (count, lanes), 1))
        return jnp.sum(jnp.where(eye, row, 0.0), axis=1, keepdims=True)

    small[0].wait()
    gain = column(gain_in[...], g_rows)

    def fold(n):
        landed(wide.at[n], ld_sem.at[n])
        for i in range(2):
            value = (wide[n, i] * gain).astype(BF16)
            for a in range(HALVES):
                part = value[:, a * q:(a + 1) * q]
                if n == last:
                    land[a, i, grow(c, me), :] = part
                else:
                    narrow[n, a, i] = part

    arrive = {}
    onward = {}

    def forward(n, a):
        block = land.at[a, :, grow(c, at[n][0]), :]
        onward[n, a] = remote(block, block, f_send.at[0], f_recv.at[a], other)
        onward[n, a].start()

    def spread(n, a):
        if n == last:
            forward(n, a)
        else:
            arrive[n, a] = remote(narrow.at[n, a], land.at[a, :, grow(c, me), :],
                                  w_send.at[0], w_recv.at[a, n], at[n][1])
            arrive[n, a].start()

    for n in range(HEAD):
        fold(n)
    met()
    for n in range(HEAD):
        spread(n, 0)

    for cp in small[1:]:
        cp.wait()

    def norm_rows(i, carry):
        r = pl.ds(pl.multiple_of(i * cap, cap), cap)
        v = tok_in[r, :].astype(f32)
        scale = lax.rsqrt(jnp.mean(v * v, axis=-1, keepdims=True) + 1e-06)
        normed[r, :] = (tok_in[r, xcols(x)].astype(f32) * scale).astype(BF16)
        return carry

    lax.fori_loop(0, GROUPS, norm_rows, 0)
    epg = gate_in.shape[0] // GROUPS
    low = ids_in[0:1, :]
    group = jnp.zeros_like(low)
    for g in range(1, GROUPS):
        group += (low >= g * epg).astype(jnp.int32)
    ahead = low == group * epg
    w_a, w_b = rw_in[0:1, :], rw_in[1:2, :]
    sub = lax.broadcasted_iota(jnp.int32, (8, tok), 0)
    w_of = jnp.where(sub == 0, jnp.where(ahead, w_a, w_b),
                     jnp.where(sub == 1, jnp.where(ahead, w_b, w_a), 0.0))
    onehot = (lax.broadcasted_iota(jnp.int32, (8, tok), 0) == group).astype(f32)
    upto = (lax.broadcasted_iota(jnp.int32, (tok, tok), 0)
            <= lax.broadcasted_iota(jnp.int32, (tok, tok), 1)).astype(BF16)
    count = jnp.dot(onehot.astype(BF16), upto, preferred_element_type=f32)
    slot = jnp.sum(onehot * count, axis=0, keepdims=True).astype(jnp.int32) - 1
    position = group * cap + slot
    spot[...] = jnp.broadcast_to(position, spot.shape)

    def picked(g):
        return lax.broadcasted_iota(jnp.int32, (cap, tok), 0) + g * cap == position

    tz, rz, ty, tx, ry = {}, {}, {}, {}, {}
    for kz in (3, 2, 1, 0):
        g = flip(z, kz)
        pick = picked(g)
        block = jnp.dot(pick.astype(BF16), normed[...], preferred_element_type=f32).astype(BF16)
        w_row = lax.dot_general(w_of, pick.astype(f32), (((1,), (1,)), ((), ())),
                                precision=lax.Precision.HIGHEST, preferred_element_type=f32)
        if kz:
            tok_s[kz - 1] = block
            rw_s[kz - 1, :, :cap] = w_row
            peer = dev(c, g, y, x)
            tz[kz] = remote(tok_s.at[kz - 1], rows.at[trow(me), xcols(x)],
                            tz_send.at[0], tz_recv.at[kz - 1], peer)
            tz[kz].start()
            rz[kz] = remote(rw_s.at[kz - 1], rw_l.at[y, z], rz_send.at[0], rz_recv.at[kz - 1], peer)
            rz[kz].start()
        else:
            rows[trow(me), xcols(x)] = block
            rw_l[y, z, :, :cap] = w_row

    def pass_x(f):
        block = rows.at[trow(f), xcols(x)]
        tx[len(tx)] = remote(block, block, tx_send.at[0], tx_recv.at[0], x_nbr)
        tx[len(tx) - 1].start()

    def pass_on(kz):
        zs = flip(z, kz)
        src = zs * n_y + y
        block = rows.at[trow(src), xcols(x)]
        ty[kz] = remote(block, block, ty_send.at[0], ty_recv.at[kz], y_nbr)
        ty[kz].start()
        pass_x(src)
        ry[kz] = remote(rw_l.at[y, zs], rw_l.at[y, zs], ry_send.at[0], ry_recv.at[0], y_nbr)
        ry[kz].start()

    pass_on(0)
    for n in range(HEAD, last + 1):
        fold(n)
        spread(n, 0)
    for n in range(last + 1):
        spread(n, 1)

    landed(dwide, dl_sem.at[0])

    def dforward(n, h):
        block = dland.at[h, drow(c, at[n][0])]
        onward[n, 2 + h] = remote(block, block, f_send.at[1], f_recv.at[2 + h], other)
        onward[n, 2 + h].start()

    for h in range(HALVES):
        for n in range(last + 1):
            value = dwide[n, :, h * piece:(h + 1) * piece].astype(BF16)
            if n == last:
                dland[h, drow(c, me)] = value
                dforward(n, h)
            else:
                dnarrow[h, n] = value
                arrive[n, 2 + h] = remote(dnarrow.at[h, n], dland.at[h, drow(c, me)],
                                          w_send.at[1], w_recv.at[2 + h, n], at[n][1])
                arrive[n, 2 + h].start()

    for kz in (1, 3, 2):
        tz[kz].wait_recv()
        rz[kz].wait_recv()
        pass_on(kz)
    for kz in (0, 1, 3, 2):
        ty[kz].wait_recv()
        pass_x(flip(z, kz) * n_y + 1 - y)

    order = sorted(range(last), key=lambda n: ks[n])

    def gather(a):
        for n in order:
            arrive[n, a].wait_recv()
            forward(n, a)
        if a == 0:
            landed(rows.at[:, xcols(1 - x)], tx_recv.at[0])
            landed(rw_l.at[1 - y], ry_recv.at[0])
        landed(land.at[a, :, core_rows(1 - c, g_rows), :], f_recv.at[a])

    m = n_y * cap
    hsend = {}
    for a in range(HALVES):
        gather(a)
        for n, kz in enumerate(RETURN):
            r = pl.ds(pl.multiple_of(flip(z, kz) * m, m), m)
            v = jnp.dot(rows[r, :], land[a, 0], preferred_element_type=f32)
            w = jnp.dot(rows[r, :], land[a, 1], preferred_element_type=f32)
            hid[x, a, r, :] = (v / (1.0 + jnp.exp(-v)) * w).astype(BF16)
            cp = remote(hid.at[x, a, r], hid.at[x, a, r], h_send.at[0], h_recv.at[a, n], x_nbr)
            cp.start()
            hsend[a, n] = cp

    part = hb // 2
    mine = pl.ds(pl.multiple_of(c * part, part), part)
    cross = []
    ysend = {}
    zsend = {}

    def give_back(n, h):
        kz = RETURN[n]
        ysend[n, h].wait_recv()
        total = (out_s[h, n, 1].astype(f32) + ry_l[h, n].astype(f32)).astype(BF16)
        d = pl.ds(h * piece, piece)
        if kz:
            fin[h, n] = total
            zsend[n, h] = remote(fin.at[h, n], ret.at[trow(z), d], z_send.at[0], z_recv.at[h],
                                 dev(c, flip(z, kz), y, x))
            zsend[n, h].start()
        else:
            ret[trow(z), d] = total

    def collect(h):
        for n in order:
            arrive[n, 2 + h].wait_recv()
            dforward(n, h)

    def project(h):
        landed(dland.at[h, core_rows(1 - c, d_rows)], f_recv.at[2 + h])
        cp = remote(dland.at[h, pl.ds(pl.multiple_of((1 - x) * hb + c * part, part), part)],
                    dcross.at[h, mine], c_send.at[0], c_recv.at[h], x_nbr)
        cp.start()
        cross.append(cp)
        for n, kz in enumerate(RETURN):
            zs = flip(z, kz)
            if h == 0:
                for a in range(HALVES):
                    hsend[a, n].wait_recv()
            for step in range(2):
                s = 1 - y if step == 0 else y
                f = zs * n_y + s
                w = jnp.where(y == 0, rw_l[s, zs, 0:1, :], rw_l[s, zs, 1:2, :])
                lane = lax.broadcasted_iota(jnp.int32, w.shape, 1)
                w = column(jnp.where(lane < cap, w, 0.0), cap)
                acc = jnp.zeros((cap, piece), f32)
                for i in range(2):
                    for a in range(HALVES):
                        acc += jnp.dot(hid[i, a, trow(f)], dland[h, pl.ds(i * hb + a * q, q)],
                                       preferred_element_type=f32)
                out_s[h, n, step] = (acc * w).astype(BF16)
                if step == 0:
                    ysend[n, h] = remote(out_s.at[h, n, 0], ry_l.at[h, n],
                                         y_send.at[0], y_recv.at[h, n], y_nbr)
                    ysend[n, h].start()

    collect(0)
    project(0)
    collect(1)
    for n in range(len(RETURN)):
        give_back(n, 0)
    project(1)
    for n in range(len(RETURN)):
        give_back(n, 1)

    over = []
    for h in range(HALVES):
        cross[h].wait_recv()
        block = dcross.at[h, mine]
        cp = remote(block, block, c_send.at[1], c_recv.at[2 + h], other)
        cp.start()
        over.append(cp)
    for h in range(HALVES):
        landed(fin.at[h, pl.ds(0, GROUPS - 1)], z_recv.at[h])
    for cp in over:
        cp.wait_recv()
    landed(narrow, w_send.at[0])
    landed(dnarrow, w_send.at[1])
    landed(land.at[:, :, core_rows(c, g_rows), :], f_send.at[0])
    landed(dland.at[:, core_rows(c, d_rows)], f_send.at[1])
    landed(tok_s, tz_send.at[0])
    landed(rw_s, rz_send.at[0])
    landed(rw_l.at[y], ry_send.at[0])
    landed(fin, ty_send.at[0])
    landed(rows.at[:, xcols(x)], tx_send.at[0])
    landed(hid.at[x], h_send.at[0])
    landed(dcross.at[:, mine], c_send.at[0])
    landed(dcross.at[:, mine], c_send.at[1])
    landed(ry_l, y_send.at[0])
    landed(fin.at[:, pl.ds(0, GROUPS - 1)], z_send.at[0])


def finish(n_z, n_y, land, dland, dcross, ret, spot, gate_out, up_out, down_out, mixed_out, mixed, sem):
    x = place(n_z, n_y)[3]
    tok, half = ret.shape
    hb, piece = dcross.shape[1:]
    q = land.shape[3]
    copies = []

    def put(src, dst):
        cp = pltpu.make_async_copy(src, dst, sem.at[len(copies)])
        cp.start()
        copies.append(cp)

    for i, out in enumerate((gate_out, up_out)):
        for a in range(HALVES):
            put(land.at[a, i], out.at[0, :, pl.ds(a * q, q)])
    for h in range(HALVES):
        put(dland.at[h, pl.ds(pl.multiple_of(x * hb, hb), hb)],
            down_out.at[0, :, pl.ds(pl.multiple_of(x * half + h * piece, piece), piece)])
        put(dcross.at[h],
            down_out.at[0, :, pl.ds(pl.multiple_of((1 - x) * half + h * piece, piece), piece)])
    everyone = (lax.broadcasted_iota(jnp.int32, (tok, tok), 0) == spot[0:1, :]).astype(BF16)
    mixed[...] = lax.dot_general(
        everyone, ret[...], (((0,), (0,)), ((), ())), preferred_element_type=jnp.float32).astype(BF16)
    put(mixed, mixed_out)
    for cp in copies:
        cp.wait()


def paired(n_z, n_y, tokens, route_ids, route_weights, norm_gain, gate_weight, up_weight, down_weight):
    tok, width = tokens.shape
    cap = tok // GROUPS
    half = width // lax.axis_size("tp")
    n_fs = n_z * n_y
    d_rows, d_cols = down_weight.shape[1:]
    g_rows, g_cols = gate_weight.shape[1:]
    f32, i32 = jnp.float32, jnp.int32
    q, piece = g_cols // HALVES, half // HALVES
    hb = n_fs * d_rows

    hbm = pl.BlockSpec(memory_space=pltpu.HBM)
    vmem = pl.BlockSpec(memory_space=pltpu.VMEM)
    dma = pltpu.SemaphoreType.DMA
    lanes = -(-cap // 128) * 128
    held = pl.pallas_call(
        functools.partial(sampler, n_z, n_y),
        out_shape=(
            pltpu.VMEM((HALVES, 2, 2 * n_fs * g_rows, q), BF16),
            pltpu.VMEM((HALVES, 2 * hb, piece), BF16),
            pltpu.VMEM((HALVES, hb, piece), BF16),
            pltpu.VMEM((tok, half), BF16),
            pltpu.VMEM((8, tok), i32),
        ),
        in_specs=[hbm] * 7,
        out_specs=(vmem,) * 5,
        scratch_shapes=[
            pltpu.VMEM((tok, width), BF16),
            pltpu.VMEM((2, tok), i32),
            pltpu.VMEM((2, tok), f32),
            pltpu.VMEM((1, g_rows), f32),
            pltpu.VMEM((n_fs, 2, g_rows, g_cols), f32),
            pltpu.VMEM((n_fs - 1, HALVES, 2, g_rows, q), BF16),
            pltpu.VMEM((n_fs, d_rows, d_cols), f32),
            pltpu.VMEM((HALVES, n_fs - 1, d_rows, piece), BF16),
            pltpu.VMEM((tok, half), BF16),
            pltpu.VMEM((3, cap, half), BF16),
            pltpu.VMEM((n_fs * cap, width), BF16),
            pltpu.VMEM((3, 8, lanes), f32),
            pltpu.VMEM((n_y, n_z, 8, lanes), f32),
            pltpu.VMEM((2, HALVES, n_fs * cap, q), BF16),
            pltpu.VMEM((HALVES, 4, 2, cap, piece), BF16),
            pltpu.VMEM((HALVES, 4, cap, piece), BF16),
            pltpu.VMEM((HALVES, 4, cap, piece), BF16),
            dma((4,)), dma((n_fs,)), dma((1,)),
            dma((2,)), dma((4, n_fs - 1)), dma((2,)), dma((4,)),
            dma((1,)), dma((3,)), dma((1,)), dma((4,)), dma((1,)), dma((1,)),
            dma((1,)), dma((3,)), dma((1,)), dma((1,)),
            dma((1,)), dma((HALVES, 4)), dma((2,)), dma((4,)),
            dma((1,)), dma((HALVES, 4)), dma((1,)), dma((2,)),
        ],
        compiler_params=pltpu.CompilerParams(
            collective_id=0, has_side_effects=True, vmem_limit_bytes=40 * 1024 * 1024),
    )(*(pltpu.with_memory_space_constraint(v, pltpu.HBM) for v in (
        tokens, route_ids.T, route_weights.T, norm_gain.reshape(1, g_rows),
        gate_weight, up_weight, down_weight)))
    return pl.pallas_call(
        functools.partial(finish, n_z, n_y),
        out_shape=(
            jax.ShapeDtypeStruct((1, 2 * n_fs * g_rows, g_cols), BF16),
            jax.ShapeDtypeStruct((1, 2 * n_fs * g_rows, g_cols), BF16),
            jax.ShapeDtypeStruct((1, hb, 2 * d_cols), BF16),
            jax.ShapeDtypeStruct((tok, half), BF16),
        ),
        in_specs=[vmem] * 5,
        out_specs=(hbm,) * 4,
        scratch_shapes=[pltpu.VMEM((tok, half), BF16), dma((9,))],
        compiler_params=pltpu.CompilerParams(vmem_limit_bytes=8 * 1024 * 1024),
    )(*(pltpu.with_memory_space_constraint(v, pltpu.VMEM) for v in held))


def solution(mesh):
    placed = (
        P(("gr", "fs"), None),
        P(("gr", "fs"), None),
        P(("gr", "fs"), None),
        P(("gr", "fs")),
        P(None, ("gr", "fs"), "tp"),
        P(None, ("gr", "fs"), "tp"),
        P(None, ("gr", "fs"), "tp"),
    )
    n_fs = mesh.shape["fs"]

    def body(*args):
        experts = args[4].shape[0]
        if experts == n_fs == 2 * GROUPS and mesh.shape["gr"] == mesh.shape["tp"] == 2:
            return paired(GROUPS, 2, *args)
        return local(*args)

    return jax.shard_map(
        body,
        mesh=mesh,
        in_specs=placed,
        out_specs=(
            P("fs", None, "tp"),
            P("fs", None, "tp"),
            P("fs", "tp", None),
            P(("gr", "fs"), "tp"),
        ),
        check_vma=False,
    )
```

```python
import functools

import jax
import jax.numpy as jnp
from jax import lax
from jax.experimental import pallas as pl
from jax.experimental.pallas import tpu as pltpu
from jax.sharding import PartitionSpec as P

GROUPS = 4
HEAD = 2
HALVES = 2
RETURN = (3, 2, 1, 0)
BF16 = jnp.bfloat16
MESH = pl.DeviceIdType.MESH


def local(tokens, route_ids, route_weights, norm_gain, gate_weight, up_weight, down_weight):
    gate_folded = (gate_weight * norm_gain[None, :, None]).astype(jnp.bfloat16)
    up_folded = (up_weight * norm_gain[None, :, None]).astype(jnp.bfloat16)
    down_rounded = down_weight.astype(jnp.bfloat16)
    moved = (
        lax.all_to_all(gate_folded, "fs", split_axis=0, concat_axis=1, tiled=True),
        lax.all_to_all(up_folded, "fs", split_axis=0, concat_axis=1, tiled=True),
        lax.all_to_all(down_rounded, "fs", split_axis=0, concat_axis=1, tiled=True),
    )
    gate_new, up_new, down_whole = (
        lax.all_gather(moved[0], "gr", axis=1, tiled=True),
        lax.all_gather(moved[1], "gr", axis=1, tiled=True),
        lax.all_gather(moved[2], "gr", axis=1, tiled=True),
    )
    down_new = lax.all_to_all(down_whole, "tp", split_axis=1, concat_axis=2, tiled=True)
    tok = tokens.shape[0]
    width = tokens.shape[1]
    experts = gate_weight.shape[0]
    cap = 2 * tok // experts
    flat_ids = route_ids.reshape(-1)
    onehot = (flat_ids[:, None] == jnp.arange(experts, dtype=jnp.int32)[None, :]).astype(jnp.int32)
    slot = jnp.sum(jnp.cumsum(onehot, axis=0) * onehot, axis=1) - 1
    position = flat_ids * cap + slot
    source = (
        jnp.zeros((experts * cap,), jnp.int32)
        .at[position]
        .set(jnp.arange(2 * tok, dtype=jnp.int32) // 2)
    )
    widened = tokens.astype(jnp.float32)
    normed = (
        widened * lax.rsqrt(jnp.mean(widened * widened, axis=-1, keepdims=True) + 1e-06)
    ).astype(jnp.bfloat16)
    outgoing = normed[source].reshape(experts, cap, width)
    received = lax.all_to_all(outgoing, "fs", split_axis=0, concat_axis=0, tiled=True)
    senders, count, _ = received.shape
    rows = received.reshape(senders * count, width)
    first = jnp.dot(rows, gate_new[0], preferred_element_type=jnp.float32)
    second = jnp.dot(rows, up_new[0], preferred_element_type=jnp.float32)
    hidden = (jax.nn.silu(first) * second).astype(jnp.bfloat16)
    partial_out = jnp.dot(hidden, down_new[0], preferred_element_type=jnp.float32)
    summed = lax.psum_scatter(
        partial_out.reshape(senders, count, width).astype(jnp.bfloat16),
        "tp",
        scatter_dimension=2,
        tiled=True,
    )
    returned = lax.all_to_all(summed, "fs", split_axis=0, concat_axis=0, tiled=True)
    columns = returned.shape[2]
    route_out = returned.reshape(experts * cap, columns)[position].reshape(tok, 2, columns)
    mixed = jnp.sum(route_weights[:, :, None] * route_out.astype(jnp.float32), axis=1).astype(
        jnp.bfloat16
    )
    return (gate_new, up_new, down_new, mixed)


def place(n_z, n_y):
    f = lax.axis_index("fs")
    return lax.axis_index("gr"), f // n_y, lax.rem(f, n_y), lax.axis_index("tp")


def flip(z, k):
    steps = (z, z + 1 - 2 * lax.rem(z, 2), lax.rem(z + 2, 4), 3 - z)
    if isinstance(k, int):
        return steps[k]
    return jnp.where(k == 1, steps[1], jnp.where(k == 2, steps[2], steps[3]))


def device(c, z, y, x, n_y):
    return {"gr": c, "fs": z * n_y + y, "tp": x}


def remote(src, dst, send, recv, peer):
    return pltpu.make_async_remote_copy(
        src_ref=src, dst_ref=dst, send_sem=send, recv_sem=recv,
        device_id=peer, device_id_type=MESH,
    )


def landed(ref, sem):
    pltpu.make_async_copy(ref, ref, sem).wait()


def sampler(
    n_z, n_y,
    tok_hbm, ids_hbm, rw_hbm, gain_hbm, gate_in, up_in, down_in,
    land, dland, dcross, ret, spot,
    tok_in, ids_in, rw_in, gain_in, wide, narrow, dwide, dnarrow,
    normed, tok_s, rows, rw_s, rw_l, hid, out_s, ry_l, fin,
    ready, in_sem, ld_sem, dl_sem, w_send, w_recv, f_send, f_recv,
    tz_send, tz_recv, ty_send, ty_recv, tx_send, tx_recv,
    rz_send, rz_recv, ry_send, ry_recv,
    h_send, h_recv, c_send, c_recv, y_send, y_recv, z_send, z_recv,
):
    c, z, y, x = place(n_z, n_y)
    me = z * n_y + y
    n_fs = n_z * n_y
    g_rows, d_rows = gate_in.shape[1], down_in.shape[1]
    tok, width = tok_in.shape
    half = width // 2
    cap = tok // GROUPS
    hb = n_fs * d_rows
    q = hb // HALVES
    piece = half // HALVES
    f32 = jnp.float32
    dev = functools.partial(device, n_y=n_y)
    outer = (z == 0) | (z == n_z - 1)
    near, far = jnp.where(outer, 1, 3), jnp.where(outer, 3, 1)
    last = n_fs - 1

    def partner(kz, ky):
        pz = flip(z, kz)
        py = 1 - y if isinstance(kz, int) and kz == 0 else lax.rem(y + ky + c, 2)
        return pz * n_y + py, dev(c, pz, py, x), kz

    at = [partner(kz, ky) for kz in (near, far, 2) for ky in range(2)]
    at += [partner(0, 1), (me, None, None)]
    peers = [partner(kz, ky) for kz in (1, 2, 3) for ky in range(2)] + [partner(0, 1)]
    other = dev(1 - c, z, y, x)
    x_nbr = dev(c, z, y, 1 - x)
    y_nbr = dev(c, z, 1 - y, x)

    def xcols(i):
        return pl.ds(pl.multiple_of(i * half, half), half)

    def grow(core, f):
        return pl.ds(pl.multiple_of((core * n_fs + f) * g_rows, g_rows), g_rows)

    def drow(core, f):
        return pl.ds(pl.multiple_of((core * n_fs + f) * d_rows, d_rows), d_rows)

    def core_rows(core, count):
        return pl.ds(pl.multiple_of(core * n_fs * count, n_fs * count), n_fs * count)

    def trow(f):
        return pl.ds(pl.multiple_of(f * cap, cap), cap)

    barrier = pltpu.get_barrier_semaphore()

    def tell(sem, peer):
        pl.semaphore_signal(sem, inc=1, device_id=peer, device_id_type=MESH)

    beside = [peers[k][1] for k in (4, 5, 6)] + [other, x_nbr]
    across = [peers[k][1] for k in range(4)]
    for peer in beside:
        tell(barrier, peer)

    @pl.when(jnp.logical_not(outer))
    def _():
        for peer in across:
            tell(barrier, peer)

    def met():
        pl.semaphore_wait(barrier, len(beside) + jnp.where(outer, len(across), 0))

        @pl.when(outer)
        def _():
            for peer in across:
                tell(ready, peer)

    small = []

    def fetch(src, dst):
        cp = pltpu.make_async_copy(src, dst, in_sem.at[len(small)])
        cp.start()
        small.append(cp)

    fetch(gain_hbm, gain_in)
    loads = {}

    def load(n):
        for i, ref in enumerate((gate_in, up_in)):
            pltpu.make_async_copy(ref.at[at[n][0]], wide.at[n, i], ld_sem.at[int(n >= HEAD)]).start()

    for n in range(HEAD):
        load(n)
    fetch(tok_hbm, tok_in)
    fetch(ids_hbm, ids_in)
    fetch(rw_hbm, rw_in)

    def column(row, count):
        lanes = row.shape[1]
        eye = (lax.broadcasted_iota(jnp.int32, (count, lanes), 0)
               == lax.broadcasted_iota(jnp.int32, (count, lanes), 1))
        return jnp.sum(jnp.where(eye, row, 0.0), axis=1, keepdims=True)

    small[0].wait()
    gain = column(gain_in[...], g_rows)

    def fold(n):
        for i in range(2):
            value = (wide[n, i] * gain).astype(BF16)
            for a in range(HALVES):
                part = value[:, a * q:(a + 1) * q]
                if n == last:
                    land[a, i, grow(c, me), :] = part
                else:
                    narrow[n, a, i] = part

    def forward(f, a):
        block = land.at[a, :, grow(c, f), :]
        remote(block, block, f_send.at[0], f_recv.at[a], other).start()

    def arrived(kz, a):
        group = [f for f, _, k in peers if k == kz]
        landed(narrow.at[pl.ds(0, len(group)), a], w_recv.at[a, kz])
        for f in group:
            forward(f, a)

    def spread(n, a):
        if n == last:
            forward(me, a)
        else:
            remote(narrow.at[n, a], land.at[a, :, grow(c, me), :],
                   w_send.at[0], w_recv.at[a, at[n][2]], at[n][1]).start()

    landed(wide.at[pl.ds(0, HEAD)], ld_sem.at[0])
    for n in range(HEAD):
        fold(n)
    met()
    for n in range(HEAD):
        spread(n, 0)
    for n in range(HEAD, last + 1):
        load(n)
    for n, (p, _, _) in enumerate(at):
        pltpu.make_async_copy(down_in.at[p], dwide.at[n], dl_sem.at[0]).start()

    for cp in small[1:]:
        cp.wait()

    def norm_rows(i, carry):
        r = pl.ds(pl.multiple_of(i * cap, cap), cap)
        v = tok_in[r, :].astype(f32)
        scale = lax.rsqrt(jnp.mean(v * v, axis=-1, keepdims=True) + 1e-06)
        normed[r, :] = (tok_in[r, xcols(x)].astype(f32) * scale).astype(BF16)
        return carry

    lax.fori_loop(0, GROUPS, norm_rows, 0)
    epg = gate_in.shape[0] // GROUPS
    low = ids_in[0:1, :]
    group = jnp.zeros_like(low)
    for g in range(1, GROUPS):
        group += (low >= g * epg).astype(jnp.int32)
    ahead = low == group * epg
    w_a, w_b = rw_in[0:1, :], rw_in[1:2, :]
    sub = lax.broadcasted_iota(jnp.int32, (8, tok), 0)
    w_of = jnp.where(sub == 0, jnp.where(ahead, w_a, w_b),
                     jnp.where(sub == 1, jnp.where(ahead, w_b, w_a), 0.0))
    onehot = (lax.broadcasted_iota(jnp.int32, (8, tok), 0) == group).astype(f32)
    upto = (lax.broadcasted_iota(jnp.int32, (tok, tok), 0)
            <= lax.broadcasted_iota(jnp.int32, (tok, tok), 1)).astype(BF16)
    count = jnp.dot(onehot.astype(BF16), upto, preferred_element_type=f32)
    slot = jnp.sum(onehot * count, axis=0, keepdims=True).astype(jnp.int32) - 1
    position = group * cap + slot
    spot[...] = jnp.broadcast_to(position, spot.shape)

    def picked(g):
        return lax.broadcasted_iota(jnp.int32, (cap, tok), 0) + g * cap == position

    def hop(kz):
        peer = dev(c, flip(z, kz), y, x)
        return (remote(tok_s.at[kz - 1], rows.at[trow(me), xcols(x)],
                       tz_send.at[0], tz_recv.at[kz - 1], peer),
                remote(rw_s.at[kz - 1], rw_l.at[y, z], rz_send.at[0], rz_recv.at[kz - 1], peer))

    for kz in (3, 2, 1, 0):
        g = flip(z, kz)
        pick = picked(g)
        block = jnp.dot(pick.astype(BF16), normed[...], preferred_element_type=f32).astype(BF16)
        w_row = lax.dot_general(w_of, pick.astype(f32), (((1,), (1,)), ((), ())),
                                precision=lax.Precision.HIGHEST, preferred_element_type=f32)
        if kz:
            tok_s[kz - 1] = block
            rw_s[kz - 1, :, :cap] = w_row[:2]
            if kz == 2:
                @pl.when(jnp.logical_not(outer))
                def _():
                    pl.semaphore_wait(ready, len(across))
            for cp in hop(kz):
                cp.start()
        else:
            rows[trow(me), xcols(x)] = block
            rw_l[y, z, :, :cap] = w_row[:2]

    def pass_x(f):
        block = rows.at[trow(f), xcols(x)]
        remote(block, block, tx_send.at[0], tx_recv.at[0], x_nbr).start()

    def pass_on(kz):
        zs = flip(z, kz)
        src = zs * n_y + y
        block = rows.at[trow(src), xcols(x)]
        remote(block, block, ty_send.at[0], ty_recv.at[kz], y_nbr).start()
        pass_x(src)
        remote(rw_l.at[y, zs], rw_l.at[y, zs], ry_send.at[0], ry_recv.at[0], y_nbr).start()

    def from_z(kz):
        for cp in hop(kz):
            cp.wait_recv()
        pass_on(kz)

    def from_y(kz):
        f = flip(z, kz) * n_y + 1 - y
        landed(rows.at[trow(f), xcols(x)], ty_recv.at[kz])
        pass_x(f)

    pass_on(0)
    landed(wide.at[pl.ds(HEAD, n_fs - HEAD)], ld_sem.at[1])
    for n in range(HEAD, last + 1):
        fold(n)
        spread(n, 0)
    for n in range(last + 1):
        spread(n, 1)

    landed(dwide, dl_sem.at[0])
    for h in range(HALVES):
        for n in range(last + 1):
            value = dwide[n, :, h * piece:(h + 1) * piece].astype(BF16)
            if n == last:
                dland[h, drow(c, me)] = value
            else:
                dnarrow[h, n] = value

    def dforward(f, h):
        block = dland.at[h, drow(c, f)]
        remote(block, block, f_send.at[1], f_recv.at[2 + h], other).start()

    def dspread():
        for h in range(HALVES):
            for n in range(last):
                remote(dnarrow.at[h, n], dland.at[h, drow(c, me)],
                       w_send.at[1], w_recv.at[2 + h, at[n][2]], at[n][1]).start()
            dforward(me, h)

    @pl.when(jnp.logical_not(outer))
    def _():
        dspread()

    early, late = jnp.where(outer, 3, 2), jnp.where(outer, 2, 3)
    from_z(early)
    from_y(0)
    from_z(1)
    from_y(early)
    from_y(1)
    from_z(late)
    from_y(late)

    def gather(a):
        for kz in range(n_z):
            arrived(kz, a)
        if a == 0:
            landed(rows.at[:, xcols(1 - x)], tx_recv.at[0])
            landed(rw_l.at[1 - y], ry_recv.at[0])
        landed(land.at[a, :, core_rows(1 - c, g_rows), :], f_recv.at[a])

    m = n_y * cap
    hsend = {}
    for a in range(HALVES):
        gather(a)
        if a == 1:
            @pl.when(outer)
            def _():
                dspread()
        for n, kz in enumerate(RETURN):
            r = pl.ds(pl.multiple_of(flip(z, kz) * m, m), m)
            v = jnp.dot(rows[r, :], land[a, 0], preferred_element_type=f32)
            w = jnp.dot(rows[r, :], land[a, 1], preferred_element_type=f32)
            hid[x, a, r, :] = (v / (1.0 + jnp.exp(-v)) * w).astype(BF16)
            cp = remote(hid.at[x, a, r], hid.at[x, a, r], h_send.at[0], h_recv.at[a, n], x_nbr)
            cp.start()
            hsend[a, n] = cp

    part = hb // 2
    mine = pl.ds(pl.multiple_of(c * part, part), part)
    cross = []
    ysend = {}

    def give_back(n, h):
        kz = RETURN[n]
        ysend[n, h].wait_recv()
        total = (out_s[h, n, 1].astype(f32) + ry_l[h, n].astype(f32)).astype(BF16)
        d = pl.ds(h * piece, piece)
        if kz:
            fin[h, n] = total
            remote(fin.at[h, n], ret.at[trow(z), d], z_send.at[0], z_recv.at[h],
                   dev(c, flip(z, kz), y, x)).start()
        else:
            ret[trow(z), d] = total

    def collect(h):
        for kz in range(n_z):
            group = [f for f, _, k in peers if k == kz]
            landed(dnarrow.at[h, pl.ds(0, len(group))], w_recv.at[2 + h, kz])
            for f in group:
                dforward(f, h)

    def project(h):
        landed(dland.at[h, core_rows(1 - c, d_rows)], f_recv.at[2 + h])
        cp = remote(dland.at[h, pl.ds(pl.multiple_of((1 - x) * hb + c * part, part), part)],
                    dcross.at[h, mine], c_send.at[0], c_recv.at[h], x_nbr)
        cp.start()
        cross.append(cp)
        for n, kz in enumerate(RETURN):
            zs = flip(z, kz)
            if h == 0:
                for a in range(HALVES):
                    hsend[a, n].wait_recv()
            for step in range(2):
                s = 1 - y if step == 0 else y
                f = zs * n_y + s
                w = jnp.where(y == 0, rw_l[s, zs, 0:1, :], rw_l[s, zs, 1:2, :])
                lane = lax.broadcasted_iota(jnp.int32, w.shape, 1)
                w = column(jnp.where(lane < cap, w, 0.0), cap)
                acc = jnp.zeros((cap, piece), f32)
                for i in range(2):
                    for a in range(HALVES):
                        acc += jnp.dot(hid[i, a, trow(f)], dland[h, pl.ds(i * hb + a * q, q)],
                                       preferred_element_type=f32)
                out_s[h, n, step] = (acc * w).astype(BF16)
                if step == 0:
                    ysend[n, h] = remote(out_s.at[h, n, 0], ry_l.at[h, n],
                                         y_send.at[0], y_recv.at[h, n], y_nbr)
                    ysend[n, h].start()

    collect(0)
    project(0)
    @pl.when(jnp.logical_not(outer))
    def _():
        give_back(0, 0)
        give_back(1, 0)

    collect(1)

    @pl.when(outer)
    def _():
        give_back(0, 0)
        give_back(1, 0)

    project(1)
    over = []

    def cross_on(h):
        cross[h].wait_recv()
        block = dcross.at[h, mine]
        cp = remote(block, block, c_send.at[1], c_recv.at[2 + h], other)
        cp.start()
        over.append(cp)

    cross_on(0)
    give_back(2, 0)
    give_back(3, 0)
    for n in range(len(RETURN)):
        if n == 3:
            cross_on(1)
        give_back(n, 1)
    for h in range(HALVES):
        landed(fin.at[h, pl.ds(0, GROUPS - 1)], z_recv.at[h])
    for cp in over:
        cp.wait_recv()
    landed(narrow, w_send.at[0])
    landed(dnarrow, w_send.at[1])
    landed(land.at[:, :, core_rows(c, g_rows), :], f_send.at[0])
    landed(dland.at[:, core_rows(c, d_rows)], f_send.at[1])
    landed(tok_s, tz_send.at[0])
    landed(rw_s, rz_send.at[0])
    landed(rw_l.at[y], ry_send.at[0])
    landed(fin, ty_send.at[0])
    landed(rows.at[:, xcols(x)], tx_send.at[0])
    landed(hid.at[x], h_send.at[0])
    landed(dcross.at[:, mine], c_send.at[0])
    landed(dcross.at[:, mine], c_send.at[1])
    landed(ry_l, y_send.at[0])
    landed(fin.at[:, pl.ds(0, GROUPS - 1)], z_send.at[0])


def finish(n_z, n_y, land, dland, dcross, ret, spot, gate_out, up_out, down_out, mixed_out, mixed, sem):
    x = place(n_z, n_y)[3]
    tok, half = ret.shape
    hb, piece = dcross.shape[1:]
    q = land.shape[3]
    copies = []

    def put(src, dst):
        cp = pltpu.make_async_copy(src, dst, sem.at[len(copies)])
        cp.start()
        copies.append(cp)

    for i, out in enumerate((gate_out, up_out)):
        for a in range(HALVES):
            put(land.at[a, i], out.at[0, :, pl.ds(a * q, q)])
    for h in range(HALVES):
        put(dland.at[h, pl.ds(pl.multiple_of(x * hb, hb), hb)],
            down_out.at[0, :, pl.ds(pl.multiple_of(x * half + h * piece, piece), piece)])
        put(dcross.at[h],
            down_out.at[0, :, pl.ds(pl.multiple_of((1 - x) * half + h * piece, piece), piece)])
    everyone = (lax.broadcasted_iota(jnp.int32, (tok, tok), 0) == spot[0:1, :]).astype(BF16)
    mixed[...] = lax.dot_general(
        everyone, ret[...], (((0,), (0,)), ((), ())), preferred_element_type=jnp.float32).astype(BF16)
    put(mixed, mixed_out)
    for cp in copies:
        cp.wait()


def paired(n_z, n_y, tokens, route_ids, route_weights, norm_gain, gate_weight, up_weight, down_weight):
    tok, width = tokens.shape
    cap = tok // GROUPS
    half = width // lax.axis_size("tp")
    n_fs = n_z * n_y
    d_rows, d_cols = down_weight.shape[1:]
    g_rows, g_cols = gate_weight.shape[1:]
    f32, i32 = jnp.float32, jnp.int32
    q, piece = g_cols // HALVES, half // HALVES
    hb = n_fs * d_rows

    hbm = pl.BlockSpec(memory_space=pltpu.HBM)
    vmem = pl.BlockSpec(memory_space=pltpu.VMEM)
    dma = pltpu.SemaphoreType.DMA
    lanes = -(-cap // 128) * 128
    held = pl.pallas_call(
        functools.partial(sampler, n_z, n_y),
        out_shape=(
            pltpu.VMEM((HALVES, 2, 2 * n_fs * g_rows, q), BF16),
            pltpu.VMEM((HALVES, 2 * hb, piece), BF16),
            pltpu.VMEM((HALVES, hb, piece), BF16),
            pltpu.VMEM((tok, half), BF16),
            pltpu.VMEM((8, tok), i32),
        ),
        in_specs=[hbm] * 7,
        out_specs=(vmem,) * 5,
        scratch_shapes=[
            pltpu.VMEM((tok, width), BF16),
            pltpu.VMEM((2, tok), i32),
            pltpu.VMEM((2, tok), f32),
            pltpu.VMEM((1, g_rows), f32),
            pltpu.VMEM((n_fs, 2, g_rows, g_cols), f32),
            pltpu.VMEM((n_fs - 1, HALVES, 2, g_rows, q), BF16),
            pltpu.VMEM((n_fs, d_rows, d_cols), f32),
            pltpu.VMEM((HALVES, n_fs - 1, d_rows, piece), BF16),
            pltpu.VMEM((tok, half), BF16),
            pltpu.VMEM((3, cap, half), BF16),
            pltpu.VMEM((n_fs * cap, width), BF16),
            pltpu.VMEM((3, 2, lanes), f32),
            pltpu.VMEM((n_y, n_z, 2, lanes), f32),
            pltpu.VMEM((2, HALVES, n_fs * cap, q), BF16),
            pltpu.VMEM((HALVES, 4, 2, cap, piece), BF16),
            pltpu.VMEM((HALVES, 4, cap, piece), BF16),
            pltpu.VMEM((HALVES, 4, cap, piece), BF16),
            pltpu.SemaphoreType.REGULAR, dma((4,)), dma((2,)), dma((1,)),
            dma((2,)), dma((4, 4)), dma((2,)), dma((4,)),
            dma((1,)), dma((3,)), dma((1,)), dma((4,)), dma((1,)), dma((1,)),
            dma((1,)), dma((3,)), dma((1,)), dma((1,)),
            dma((1,)), dma((HALVES, 4)), dma((2,)), dma((4,)),
            dma((1,)), dma((HALVES, 4)), dma((1,)), dma((2,)),
        ],
        compiler_params=pltpu.CompilerParams(
            collective_id=0, has_side_effects=True, vmem_limit_bytes=40 * 1024 * 1024),
    )(*(pltpu.with_memory_space_constraint(v, pltpu.HBM) for v in (
        tokens, route_ids.T, route_weights.T, norm_gain.reshape(1, g_rows),
        gate_weight, up_weight, down_weight)))
    return pl.pallas_call(
        functools.partial(finish, n_z, n_y),
        out_shape=(
            jax.ShapeDtypeStruct((1, 2 * n_fs * g_rows, g_cols), BF16),
            jax.ShapeDtypeStruct((1, 2 * n_fs * g_rows, g_cols), BF16),
            jax.ShapeDtypeStruct((1, hb, 2 * d_cols), BF16),
            jax.ShapeDtypeStruct((tok, half), BF16),
        ),
        in_specs=[vmem] * 5,
        out_specs=(hbm,) * 4,
        scratch_shapes=[pltpu.VMEM((tok, half), BF16), dma((9,))],
        compiler_params=pltpu.CompilerParams(vmem_limit_bytes=8 * 1024 * 1024),
    )(*(pltpu.with_memory_space_constraint(v, pltpu.VMEM) for v in held))


def solution(mesh):
    placed = (
        P(("gr", "fs"), None),
        P(("gr", "fs"), None),
        P(("gr", "fs"), None),
        P(("gr", "fs")),
        P(None, ("gr", "fs"), "tp"),
        P(None, ("gr", "fs"), "tp"),
        P(None, ("gr", "fs"), "tp"),
    )
    n_fs = mesh.shape["fs"]

    def body(*args):
        experts = args[4].shape[0]
        if experts == n_fs == 2 * GROUPS and mesh.shape["gr"] == mesh.shape["tp"] == 2:
            return paired(GROUPS, 2, *args)
        return local(*args)

    return jax.shard_map(
        body,
        mesh=mesh,
        in_specs=placed,
        out_specs=(
            P("fs", None, "tp"),
            P("fs", None, "tp"),
            P("fs", "tp", None),
            P(("gr", "fs"), "tp"),
        ),
        check_vma=False,
    )
```

```python
import functools

import jax
import jax.numpy as jnp
from jax import lax
from jax.experimental import pallas as pl
from jax.experimental.pallas import tpu as pltpu
from jax.sharding import PartitionSpec as P

GROUPS = 4
HEAD = 2
HALVES = 2
BF16 = jnp.bfloat16
MESH = pl.DeviceIdType.MESH


def local(tokens, route_ids, route_weights, norm_gain, gate_weight, up_weight, down_weight):
    gate_folded = (gate_weight * norm_gain[None, :, None]).astype(jnp.bfloat16)
    up_folded = (up_weight * norm_gain[None, :, None]).astype(jnp.bfloat16)
    down_rounded = down_weight.astype(jnp.bfloat16)
    moved = (
        lax.all_to_all(gate_folded, "fs", split_axis=0, concat_axis=1, tiled=True),
        lax.all_to_all(up_folded, "fs", split_axis=0, concat_axis=1, tiled=True),
        lax.all_to_all(down_rounded, "fs", split_axis=0, concat_axis=1, tiled=True),
    )
    gate_new, up_new, down_whole = (
        lax.all_gather(moved[0], "gr", axis=1, tiled=True),
        lax.all_gather(moved[1], "gr", axis=1, tiled=True),
        lax.all_gather(moved[2], "gr", axis=1, tiled=True),
    )
    down_new = lax.all_to_all(down_whole, "tp", split_axis=1, concat_axis=2, tiled=True)
    tok = tokens.shape[0]
    width = tokens.shape[1]
    experts = gate_weight.shape[0]
    cap = 2 * tok // experts
    flat_ids = route_ids.reshape(-1)
    onehot = (flat_ids[:, None] == jnp.arange(experts, dtype=jnp.int32)[None, :]).astype(jnp.int32)
    slot = jnp.sum(jnp.cumsum(onehot, axis=0) * onehot, axis=1) - 1
    position = flat_ids * cap + slot
    source = (
        jnp.zeros((experts * cap,), jnp.int32)
        .at[position]
        .set(jnp.arange(2 * tok, dtype=jnp.int32) // 2)
    )
    widened = tokens.astype(jnp.float32)
    normed = (
        widened * lax.rsqrt(jnp.mean(widened * widened, axis=-1, keepdims=True) + 1e-06)
    ).astype(jnp.bfloat16)
    outgoing = normed[source].reshape(experts, cap, width)
    received = lax.all_to_all(outgoing, "fs", split_axis=0, concat_axis=0, tiled=True)
    senders, count, _ = received.shape
    rows = received.reshape(senders * count, width)
    first = jnp.dot(rows, gate_new[0], preferred_element_type=jnp.float32)
    second = jnp.dot(rows, up_new[0], preferred_element_type=jnp.float32)
    hidden = (jax.nn.silu(first) * second).astype(jnp.bfloat16)
    partial_out = jnp.dot(hidden, down_new[0], preferred_element_type=jnp.float32)
    summed = lax.psum_scatter(
        partial_out.reshape(senders, count, width).astype(jnp.bfloat16),
        "tp",
        scatter_dimension=2,
        tiled=True,
    )
    returned = lax.all_to_all(summed, "fs", split_axis=0, concat_axis=0, tiled=True)
    columns = returned.shape[2]
    route_out = returned.reshape(experts * cap, columns)[position].reshape(tok, 2, columns)
    mixed = jnp.sum(route_weights[:, :, None] * route_out.astype(jnp.float32), axis=1).astype(
        jnp.bfloat16
    )
    return (gate_new, up_new, down_new, mixed)


def place(n_z, n_y):
    f = lax.axis_index("fs")
    return lax.axis_index("gr"), f // n_y, lax.rem(f, n_y), lax.axis_index("tp")


def flip(z, k):
    steps = (z, z + 1 - 2 * lax.rem(z, 2), lax.rem(z + 2, 4), 3 - z)
    if isinstance(k, int):
        return steps[k]
    return jnp.where(k == 1, steps[1], jnp.where(k == 2, steps[2], steps[3]))


def device(c, z, y, x, n_y):
    return {"gr": c, "fs": z * n_y + y, "tp": x}


def remote(src, dst, send, recv, peer):
    return pltpu.make_async_remote_copy(
        src_ref=src, dst_ref=dst, send_sem=send, recv_sem=recv,
        device_id=peer, device_id_type=MESH,
    )


def landed(ref, sem):
    pltpu.make_async_copy(ref, ref, sem).wait()


def sampler(
    n_z, n_y,
    tok_hbm, ids_hbm, rw_hbm, gain_hbm, gate_in, up_in, down_in,
    land, dland, dcross, ret, spot,
    tok_in, ids_in, rw_in, gain_in, wide, narrow, dwide, dnarrow,
    normed, tok_s, rows, rw_s, rw_l, hid, out_s, ry_l, fin,
    ready, in_sem, ld_sem, dl_sem, w_send, w_recv, f_send, f_recv,
    tz_send, tz_recv, ty_send, ty_recv, tx_send, tx_recv,
    rz_send, rz_recv, ry_send, ry_recv,
    h_send, h_recv, c_send, c_recv, y_send, y_recv, z_send, z_recv,
):
    c, z, y, x = place(n_z, n_y)
    me = z * n_y + y
    n_fs = n_z * n_y
    g_rows, d_rows = gate_in.shape[1], down_in.shape[1]
    tok, width = tok_in.shape
    half = width // 2
    cap = tok // GROUPS
    hb = n_fs * d_rows
    q = hb // HALVES
    piece = half // HALVES
    f32 = jnp.float32
    dev = functools.partial(device, n_y=n_y)
    outer = (z == 0) | (z == n_z - 1)
    near, far = jnp.where(outer, 1, 3), jnp.where(outer, 3, 1)
    last = n_fs - 1

    def partner(kz, ky):
        pz = flip(z, kz)
        py = 1 - y if isinstance(kz, int) and kz == 0 else lax.rem(y + ky + c, 2)
        return pz * n_y + py, dev(c, pz, py, x), kz

    at = [partner(kz, ky) for kz in (near, far, 2) for ky in range(2)]
    at += [partner(0, 1), (me, None, None)]
    peers = [partner(kz, ky) for kz in (1, 2, 3) for ky in range(2)] + [partner(0, 1)]
    other = dev(1 - c, z, y, x)
    x_nbr = dev(c, z, y, 1 - x)
    y_nbr = dev(c, z, 1 - y, x)

    def xcols(i):
        return pl.ds(pl.multiple_of(i * half, half), half)

    def grow(core, f):
        return pl.ds(pl.multiple_of((core * n_fs + f) * g_rows, g_rows), g_rows)

    def drow(core, f):
        return pl.ds(pl.multiple_of((core * n_fs + f) * d_rows, d_rows), d_rows)

    def core_rows(core, count):
        return pl.ds(pl.multiple_of(core * n_fs * count, n_fs * count), n_fs * count)

    def trow(f):
        return pl.ds(pl.multiple_of(f * cap, cap), cap)

    small = []

    def fetch(src, dst):
        cp = pltpu.make_async_copy(src, dst, in_sem.at[len(small)])
        cp.start()
        small.append(cp)

    fetch(gain_hbm, gain_in)

    def load(n):
        for i, ref in enumerate((gate_in, up_in)):
            pltpu.make_async_copy(ref.at[at[n][0]], wide.at[n, i], ld_sem.at[int(n >= HEAD)]).start()

    for n in range(HEAD):
        load(n)
    barrier = pltpu.get_barrier_semaphore()

    def tell(sem, peer):
        pl.semaphore_signal(sem, inc=1, device_id=peer, device_id_type=MESH)

    beside = [peers[k][1] for k in (4, 5, 6)] + [other, x_nbr]
    across = [peers[k][1] for k in range(4)]
    for peer in beside:
        tell(barrier, peer)

    @pl.when(jnp.logical_not(outer))
    def _():
        for peer in across:
            tell(barrier, peer)

    fetch(tok_hbm, tok_in)
    fetch(ids_hbm, ids_in)
    fetch(rw_hbm, rw_in)

    def met():
        pl.semaphore_wait(barrier, len(beside) + jnp.where(outer, len(across), 0))

        @pl.when(outer)
        def _():
            for peer in across:
                tell(ready, peer)

    def column(row, count):
        lanes = row.shape[1]
        eye = (lax.broadcasted_iota(jnp.int32, (count, lanes), 0)
               == lax.broadcasted_iota(jnp.int32, (count, lanes), 1))
        return jnp.sum(jnp.where(eye, row, 0.0), axis=1, keepdims=True)

    small[0].wait()
    gain = column(gain_in[...], g_rows)

    def fold(n):
        for i in range(2):
            value = (wide[n, i] * gain).astype(BF16)
            for a in range(HALVES):
                part = value[:, a * q:(a + 1) * q]
                if n == last:
                    land[a, i, grow(c, me), :] = part
                else:
                    narrow[n, a, i] = part

    def forward(f, a):
        block = land.at[a, :, grow(c, f), :]
        remote(block, block, f_send.at[0], f_recv.at[a], other).start()

    def arrived(kz, a):
        group = [f for f, _, k in peers if k == kz]
        landed(narrow.at[pl.ds(0, len(group)), a], w_recv.at[a, kz])
        for f in group:
            forward(f, a)

    def spread(n, a):
        if n == last:
            forward(me, a)
        else:
            remote(narrow.at[n, a], land.at[a, :, grow(c, me), :],
                   w_send.at[0], w_recv.at[a, at[n][2]], at[n][1]).start()

    landed(wide.at[pl.ds(0, HEAD)], ld_sem.at[0])
    for n in range(HEAD):
        fold(n)
    met()
    for n in range(HEAD):
        spread(n, 0)
    for n in range(HEAD, last + 1):
        load(n)
    for n, (p, _, _) in enumerate(at):
        pltpu.make_async_copy(down_in.at[p], dwide.at[n], dl_sem.at[0]).start()

    for cp in small[1:]:
        cp.wait()

    def norm_rows(i, carry):
        r = pl.ds(pl.multiple_of(i * cap, cap), cap)
        v = tok_in[r, :].astype(f32)
        scale = lax.rsqrt(jnp.mean(v * v, axis=-1, keepdims=True) + 1e-06)
        normed[r, :] = (tok_in[r, xcols(x)].astype(f32) * scale).astype(BF16)
        return carry

    lax.fori_loop(0, GROUPS, norm_rows, 0)
    epg = gate_in.shape[0] // GROUPS
    low = ids_in[0:1, :]
    group = jnp.zeros_like(low)
    for g in range(1, GROUPS):
        group += (low >= g * epg).astype(jnp.int32)
    ahead = low == group * epg
    w_a, w_b = rw_in[0:1, :], rw_in[1:2, :]
    sub = lax.broadcasted_iota(jnp.int32, (8, tok), 0)
    w_of = jnp.where(sub == 0, jnp.where(ahead, w_a, w_b),
                     jnp.where(sub == 1, jnp.where(ahead, w_b, w_a), 0.0))
    onehot = (lax.broadcasted_iota(jnp.int32, (8, tok), 0) == group).astype(f32)
    upto = (lax.broadcasted_iota(jnp.int32, (tok, tok), 0)
            <= lax.broadcasted_iota(jnp.int32, (tok, tok), 1)).astype(BF16)
    count = jnp.dot(onehot.astype(BF16), upto, preferred_element_type=f32)
    slot = jnp.sum(onehot * count, axis=0, keepdims=True).astype(jnp.int32) - 1
    position = group * cap + slot
    spot[...] = jnp.broadcast_to(position, spot.shape)

    def picked(g):
        return lax.broadcasted_iota(jnp.int32, (cap, tok), 0) + g * cap == position

    def hop(kz):
        peer = dev(c, flip(z, kz), y, x)
        return (remote(tok_s.at[kz - 1], rows.at[trow(me), xcols(x)],
                       tz_send.at[0], tz_recv.at[kz - 1], peer),
                remote(rw_s.at[kz - 1], rw_l.at[y, z], rz_send.at[0], rz_recv.at[kz - 1], peer))

    for kz in (3, 2, 1, 0):
        g = flip(z, kz)
        pick = picked(g)
        block = jnp.dot(pick.astype(BF16), normed[...], preferred_element_type=f32).astype(BF16)
        w_row = lax.dot_general(w_of, pick.astype(f32), (((1,), (1,)), ((), ())),
                                precision=lax.Precision.HIGHEST, preferred_element_type=f32)
        if kz:
            tok_s[kz - 1] = block
            rw_s[kz - 1, :, :cap] = w_row[:2]
            if kz == 2:
                @pl.when(jnp.logical_not(outer))
                def _():
                    pl.semaphore_wait(ready, len(across))
            for cp in hop(kz):
                cp.start()
        else:
            rows[trow(me), xcols(x)] = block
            rw_l[y, z, :, :cap] = w_row[:2]

    def pass_x(f):
        block = rows.at[trow(f), xcols(x)]
        remote(block, block, tx_send.at[0], tx_recv.at[0], x_nbr).start()

    def pass_on(kz):
        zs = flip(z, kz)
        src = zs * n_y + y
        block = rows.at[trow(src), xcols(x)]
        remote(block, block, ty_send.at[0], ty_recv.at[kz], y_nbr).start()
        pass_x(src)
        remote(rw_l.at[y, zs], rw_l.at[y, zs], ry_send.at[0], ry_recv.at[0], y_nbr).start()

    def from_z(kz):
        for cp in hop(kz):
            cp.wait_recv()
        pass_on(kz)

    def from_y(kz):
        f = flip(z, kz) * n_y + 1 - y
        landed(rows.at[trow(f), xcols(x)], ty_recv.at[kz])
        pass_x(f)

    pass_on(0)
    landed(wide.at[pl.ds(HEAD, n_fs - HEAD)], ld_sem.at[1])
    for n in range(HEAD, last + 1):
        fold(n)
        spread(n, 0)
    for n in range(last + 1):
        spread(n, 1)

    landed(dwide, dl_sem.at[0])
    for h in range(HALVES):
        for n in range(last + 1):
            value = dwide[n, :, h * piece:(h + 1) * piece].astype(BF16)
            if n == last:
                dland[h, drow(c, me)] = value
            else:
                dnarrow[h, n] = value

    def dforward(f, h):
        block = dland.at[h, drow(c, f)]
        remote(block, block, f_send.at[1], f_recv.at[2 + h], other).start()

    def dspread():
        for h in range(HALVES):
            for n in range(last):
                remote(dnarrow.at[h, n], dland.at[h, drow(c, me)],
                       w_send.at[1], w_recv.at[2 + h, at[n][2]], at[n][1]).start()
            dforward(me, h)

    @pl.when(jnp.logical_not(outer))
    def _():
        dspread()

    early, late = jnp.where(outer, 3, 2), jnp.where(outer, 2, 3)
    from_z(early)
    from_y(0)
    from_z(1)
    from_y(early)
    from_y(1)
    from_z(late)
    from_y(late)

    def gather(a):
        for kz in range(n_z):
            arrived(kz, a)
        if a == 0:
            landed(rows.at[:, xcols(1 - x)], tx_recv.at[0])
            landed(rw_l.at[1 - y], ry_recv.at[0])
        landed(land.at[a, :, core_rows(1 - c, g_rows), :], f_recv.at[a])

    m = n_y * cap
    back = (early, late, 1, 0)
    hsend = {}
    for a in range(HALVES):
        gather(a)
        if a == 1:
            @pl.when(outer)
            def _():
                dspread()
        for n, kz in enumerate(back):
            r = pl.ds(pl.multiple_of(flip(z, kz) * m, m), m)
            v = jnp.dot(rows[r, :], land[a, 0], preferred_element_type=f32)
            w = jnp.dot(rows[r, :], land[a, 1], preferred_element_type=f32)
            hid[x, a, r, :] = (v / (1.0 + jnp.exp(-v)) * w).astype(BF16)
            cp = remote(hid.at[x, a, r], hid.at[x, a, r], h_send.at[0], h_recv.at[a, n], x_nbr)
            cp.start()
            hsend[a, n] = cp

    part = hb // 2
    mine = pl.ds(pl.multiple_of(c * part, part), part)
    cross = []
    ysend = {}

    def give_back(n, h):
        kz = back[n]
        ysend[n, h].wait_recv()
        total = (out_s[h, n, 1].astype(f32) + ry_l[h, n].astype(f32)).astype(BF16)
        d = pl.ds(h * piece, piece)
        if n < 3:
            fin[h, n] = total
            remote(fin.at[h, n], ret.at[trow(z), d], z_send.at[0], z_recv.at[h],
                   dev(c, flip(z, kz), y, x)).start()
        else:
            ret[trow(z), d] = total

    def collect(h):
        for kz in range(n_z):
            group = [f for f, _, k in peers if k == kz]
            landed(dnarrow.at[h, pl.ds(0, len(group))], w_recv.at[2 + h, kz])
            for f in group:
                dforward(f, h)

    def project(h):
        landed(dland.at[h, core_rows(1 - c, d_rows)], f_recv.at[2 + h])
        cp = remote(dland.at[h, pl.ds(pl.multiple_of((1 - x) * hb + c * part, part), part)],
                    dcross.at[h, mine], c_send.at[0], c_recv.at[h], x_nbr)
        cp.start()
        cross.append(cp)
        for n, kz in enumerate(back):
            zs = flip(z, kz)
            if h == 0:
                for a in range(HALVES):
                    hsend[a, n].wait_recv()
            for step in range(2):
                s = 1 - y if step == 0 else y
                f = zs * n_y + s
                w = jnp.where(y == 0, rw_l[s, zs, 0:1, :], rw_l[s, zs, 1:2, :])
                lane = lax.broadcasted_iota(jnp.int32, w.shape, 1)
                w = column(jnp.where(lane < cap, w, 0.0), cap)
                acc = jnp.zeros((cap, piece), f32)
                for i in range(2):
                    for a in range(HALVES):
                        acc += jnp.dot(hid[i, a, trow(f)], dland[h, pl.ds(i * hb + a * q, q)],
                                       preferred_element_type=f32)
                out_s[h, n, step] = (acc * w).astype(BF16)
                if step == 0:
                    ysend[n, h] = remote(out_s.at[h, n, 0], ry_l.at[h, n],
                                         y_send.at[0], y_recv.at[h, n], y_nbr)
                    ysend[n, h].start()

    collect(0)
    project(0)
    @pl.when(jnp.logical_not(outer))
    def _():
        give_back(0, 0)
        give_back(1, 0)

    collect(1)

    @pl.when(outer)
    def _():
        give_back(0, 0)
        give_back(1, 0)

    project(1)
    over = []

    def cross_on(h):
        cross[h].wait_recv()
        block = dcross.at[h, mine]
        cp = remote(block, block, c_send.at[1], c_recv.at[2 + h], other)
        cp.start()
        over.append(cp)

    cross_on(0)
    give_back(2, 0)
    give_back(3, 0)
    for n in range(len(back)):
        if n == 3:
            cross_on(1)
        give_back(n, 1)
    for h in range(HALVES):
        landed(fin.at[h, pl.ds(0, GROUPS - 1)], z_recv.at[h])
    for cp in over:
        cp.wait_recv()
    landed(narrow, w_send.at[0])
    landed(dnarrow, w_send.at[1])
    landed(land.at[:, :, core_rows(c, g_rows), :], f_send.at[0])
    landed(dland.at[:, core_rows(c, d_rows)], f_send.at[1])
    landed(tok_s, tz_send.at[0])
    landed(rw_s, rz_send.at[0])
    landed(rw_l.at[y], ry_send.at[0])
    landed(fin, ty_send.at[0])
    landed(rows.at[:, xcols(x)], tx_send.at[0])
    landed(hid.at[x], h_send.at[0])
    landed(dcross.at[:, mine], c_send.at[0])
    landed(dcross.at[:, mine], c_send.at[1])
    landed(ry_l, y_send.at[0])
    landed(fin.at[:, pl.ds(0, GROUPS - 1)], z_send.at[0])


def finish(n_z, n_y, land, dland, dcross, ret, spot, gate_out, up_out, down_out, mixed_out, mixed, sem):
    x = place(n_z, n_y)[3]
    tok, half = ret.shape
    hb, piece = dcross.shape[1:]
    q = land.shape[3]
    copies = []

    def put(src, dst):
        cp = pltpu.make_async_copy(src, dst, sem.at[len(copies)])
        cp.start()
        copies.append(cp)

    for i, out in enumerate((gate_out, up_out)):
        for a in range(HALVES):
            put(land.at[a, i], out.at[0, :, pl.ds(a * q, q)])
    for h in range(HALVES):
        put(dland.at[h, pl.ds(pl.multiple_of(x * hb, hb), hb)],
            down_out.at[0, :, pl.ds(pl.multiple_of(x * half + h * piece, piece), piece)])
        put(dcross.at[h],
            down_out.at[0, :, pl.ds(pl.multiple_of((1 - x) * half + h * piece, piece), piece)])
    everyone = (lax.broadcasted_iota(jnp.int32, (tok, tok), 0) == spot[0:1, :]).astype(BF16)
    mixed[...] = lax.dot_general(
        everyone, ret[...], (((0,), (0,)), ((), ())), preferred_element_type=jnp.float32).astype(BF16)
    put(mixed, mixed_out)
    for cp in copies:
        cp.wait()


def paired(n_z, n_y, tokens, route_ids, route_weights, norm_gain, gate_weight, up_weight, down_weight):
    tok, width = tokens.shape
    cap = tok // GROUPS
    half = width // lax.axis_size("tp")
    n_fs = n_z * n_y
    d_rows, d_cols = down_weight.shape[1:]
    g_rows, g_cols = gate_weight.shape[1:]
    f32, i32 = jnp.float32, jnp.int32
    q, piece = g_cols // HALVES, half // HALVES
    hb = n_fs * d_rows

    hbm = pl.BlockSpec(memory_space=pltpu.HBM)
    vmem = pl.BlockSpec(memory_space=pltpu.VMEM)
    dma = pltpu.SemaphoreType.DMA
    lanes = -(-cap // 128) * 128
    held = pl.pallas_call(
        functools.partial(sampler, n_z, n_y),
        out_shape=(
            pltpu.VMEM((HALVES, 2, 2 * n_fs * g_rows, q), BF16),
            pltpu.VMEM((HALVES, 2 * hb, piece), BF16),
            pltpu.VMEM((HALVES, hb, piece), BF16),
            pltpu.VMEM((tok, half), BF16),
            pltpu.VMEM((8, tok), i32),
        ),
        in_specs=[hbm] * 7,
        out_specs=(vmem,) * 5,
        scratch_shapes=[
            pltpu.VMEM((tok, width), BF16),
            pltpu.VMEM((2, tok), i32),
            pltpu.VMEM((2, tok), f32),
            pltpu.VMEM((1, g_rows), f32),
            pltpu.VMEM((n_fs, 2, g_rows, g_cols), f32),
            pltpu.VMEM((n_fs - 1, HALVES, 2, g_rows, q), BF16),
            pltpu.VMEM((n_fs, d_rows, d_cols), f32),
            pltpu.VMEM((HALVES, n_fs - 1, d_rows, piece), BF16),
            pltpu.VMEM((tok, half), BF16),
            pltpu.VMEM((3, cap, half), BF16),
            pltpu.VMEM((n_fs * cap, width), BF16),
            pltpu.VMEM((3, 2, lanes), f32),
            pltpu.VMEM((n_y, n_z, 2, lanes), f32),
            pltpu.VMEM((2, HALVES, n_fs * cap, q), BF16),
            pltpu.VMEM((HALVES, 4, 2, cap, piece), BF16),
            pltpu.VMEM((HALVES, 4, cap, piece), BF16),
            pltpu.VMEM((HALVES, 4, cap, piece), BF16),
            pltpu.SemaphoreType.REGULAR, dma((4,)), dma((2,)), dma((1,)),
            dma((2,)), dma((4, 4)), dma((2,)), dma((4,)),
            dma((1,)), dma((3,)), dma((1,)), dma((4,)), dma((1,)), dma((1,)),
            dma((1,)), dma((3,)), dma((1,)), dma((1,)),
            dma((1,)), dma((HALVES, 4)), dma((2,)), dma((4,)),
            dma((1,)), dma((HALVES, 4)), dma((1,)), dma((2,)),
        ],
        compiler_params=pltpu.CompilerParams(
            collective_id=0, has_side_effects=True, vmem_limit_bytes=40 * 1024 * 1024),
    )(*(pltpu.with_memory_space_constraint(v, pltpu.HBM) for v in (
        tokens, route_ids.T, route_weights.T, norm_gain.reshape(1, g_rows),
        gate_weight, up_weight, down_weight)))
    return pl.pallas_call(
        functools.partial(finish, n_z, n_y),
        out_shape=(
            jax.ShapeDtypeStruct((1, 2 * n_fs * g_rows, g_cols), BF16),
            jax.ShapeDtypeStruct((1, 2 * n_fs * g_rows, g_cols), BF16),
            jax.ShapeDtypeStruct((1, hb, 2 * d_cols), BF16),
            jax.ShapeDtypeStruct((tok, half), BF16),
        ),
        in_specs=[vmem] * 5,
        out_specs=(hbm,) * 4,
        scratch_shapes=[pltpu.VMEM((tok, half), BF16), dma((9,))],
        compiler_params=pltpu.CompilerParams(vmem_limit_bytes=8 * 1024 * 1024),
    )(*(pltpu.with_memory_space_constraint(v, pltpu.VMEM) for v in held))


def solution(mesh):
    placed = (
        P(("gr", "fs"), None),
        P(("gr", "fs"), None),
        P(("gr", "fs"), None),
        P(("gr", "fs")),
        P(None, ("gr", "fs"), "tp"),
        P(None, ("gr", "fs"), "tp"),
        P(None, ("gr", "fs"), "tp"),
    )
    n_fs = mesh.shape["fs"]

    def body(*args):
        experts = args[4].shape[0]
        if experts == n_fs == 2 * GROUPS and mesh.shape["gr"] == mesh.shape["tp"] == 2:
            return paired(GROUPS, 2, *args)
        return local(*args)

    return jax.shard_map(
        body,
        mesh=mesh,
        in_specs=placed,
        out_specs=(
            P("fs", None, "tp"),
            P("fs", None, "tp"),
            P("fs", "tp", None),
            P(("gr", "fs"), "tp"),
        ),
        check_vma=False,
    )
```
